256 devices in a mesh: rep: 2 (over z_hi), fs: 16 (over z_lo, y), tp: 8 (over x, core).
Axes of the slice: x: 4, y: 4, z: 8 (z_hi: 2, z_lo: 4; z = z_hi * 4 + z_lo), core: 2. Of those that a mesh axis runs over, the one named last changes fastest.
Arguments:
- inputs: bfloat16 [16384, 2048], P(('rep', 'fs')), may hold values from -6 to 6
- cotangent: bfloat16 [16384, 2048], P(('rep', 'fs')), may hold values from -6 to 6
- gate_pre: bfloat16 [16384, 5632], P(('rep', 'fs'), 'tp'), may hold values from -8 to 8
- up_pre: bfloat16 [16384, 5632], P(('rep', 'fs'), 'tp'), may hold values from -6 to 6
- gate_weight: float32 [2048, 5632], P('fs', 'tp'), may hold values from -0.125 to 0.125
- up_weight: float32 [2048, 5632], P('fs', 'tp'), may hold values from -0.125 to 0.125
- down_weight: float32 [2048, 5632], P('fs', 'tp'), may hold values from -0.078125 to 0.078125
- gate_scale: float32 [1, 5632], P(None, 'tp'), may hold values from 0.1 to 1.9
- up_scale: float32 [1, 5632], P(None, 'tp'), may hold values from 0.1 to 1.9
- down_scale: float32 [1, 5632], P(None, 'tp'), may hold values from 0.1 to 1.9
Outputs:
- input_grad: bfloat16 [16384, 2048], P(('rep', 'fs'), 'tp')
- gate_grad: float32 [2048, 5632], P('fs', 'tp')
- up_grad: float32 [2048, 5632], P('fs', 'tp')
- down_grad: float32 [2048, 5632], P('fs', 'tp')
The draws below stay inside these ranges and needn't reach their ends.
All inputs are finite; a program needn't handle non-finite values.
Results may differ from the reference program's by a relative error of at most 0.018.
Values may be sent and summed in bfloat16 or wider, within the bound.
A program may use at most 128 MiB of HBM per device.

```python
import jax
import jax.numpy as jnp
from jax import lax

D = 2048
FF = 5632
TOKENS = 16384
N_TP = 8


def spiked(array, own_key, source, target, blocks, factor):
    owner, partner = [(jnp.arange(array.shape[position]) // (array.shape[position] // blocks)).reshape([-1 if axis == position else 1 for axis in range(array.ndim)]) for position in (source, target)]
    chosen = jax.random.permutation(own_key, blocks)[partner]
    strong = (owner == chosen) | (owner == (partner + blocks // 2) % blocks)
    return jnp.where(strong, factor * array, array)


def level_of(key, extent, shards, least, top_value):
    factor_of, own = 1.0, jax.random.fold_in(key, 6)
    for axis_at, parts in shards:
        draws = jnp.exp(jax.random.uniform(jax.random.fold_in(own, axis_at), (parts,), jnp.float32, least / len(shards), top_value / len(shards)))
        factor_of = factor_of * jnp.repeat(draws, extent[axis_at] // parts).reshape([-1 if axis == axis_at else 1 for axis in range(len(extent))])
    return factor_of


def normal_values(own_key, extent, scale, reach, shards=(), kind=jnp.bfloat16):
    level = level_of(own_key, extent, shards, -0.22, 0.18) if shards else 1.0
    entries = jax.random.normal(own_key, extent, jnp.float32) * scale * level
    return jnp.minimum(jnp.maximum(entries, -reach), reach).astype(kind)


def heavy_noise(own_key, extent, deviation, reach, pieces, heavy, kind=jnp.bfloat16):
    result = deviation * jax.random.normal(own_key, extent, jnp.float32)
    if pieces:
        result = result * level_of(own_key, extent, pieces, -0.22, 0.18)
    return jnp.clip(spiked(result, jax.random.fold_in(own_key, 3), *heavy), -reach, reach).astype(kind)


def setup_inputs(seed: int = 0) -> dict:
    arg_keys = jax.random.split(jax.random.key(seed), 11)
    inputs = normal_values(arg_keys[0], (TOKENS, D), 1.0, 6.0, ((0, 32),))
    cotangent = heavy_noise(arg_keys[1], (TOKENS, D), 1.0, 6.0, ((0, 32),), (0, 1, 32, 2.75))
    gate_pre = normal_values(arg_keys[2], (TOKENS, FF), 1.5, 8.0, ((0, 32), (1, 8)))
    up_pre = normal_values(arg_keys[3], (TOKENS, FF), 1.0, 6.0, ((0, 32), (1, 8)))
    gate_weight = normal_values(arg_keys[4], (D, FF), D ** -0.5, 0.125, ((0, 16), (1, 8)), jnp.float32)
    up_weight = normal_values(arg_keys[5], (D, FF), D ** -0.5, 0.125, ((0, 16), (1, 8)), jnp.float32)
    down_weight = normal_values(arg_keys[6], (D, FF), FF ** -0.5, 0.078125, ((0, 16), (1, 8)), jnp.float32)
    gate_scale = jnp.clip(1.0 + 0.18 * jax.random.normal(arg_keys[7], (1, FF), jnp.float32), 0.1, 1.9)
    up_scale = jnp.clip(1.0 + 0.18 * jax.random.normal(arg_keys[8], (1, FF), jnp.float32), 0.1, 1.9)
    down_scale = jnp.clip(1.0 + 0.18 * jax.random.normal(arg_keys[9], (1, FF), jnp.float32), 0.1, 1.9)
    return dict(inputs=inputs, cotangent=cotangent, gate_pre=gate_pre, up_pre=up_pre, gate_weight=gate_weight, up_weight=up_weight, down_weight=down_weight, gate_scale=gate_scale, up_scale=up_scale, down_scale=down_scale)


def reference(inputs, cotangent, gate_pre, up_pre, gate_weight, up_weight, down_weight, gate_scale, up_scale, down_scale):
    gate = gate_pre.astype(jnp.float32)
    upper = up_pre.astype(jnp.float32)
    sig = jax.nn.sigmoid(gate)
    act = gate * sig
    hidden = (act * upper).astype(jnp.bfloat16)
    down_bf = down_weight.astype(jnp.bfloat16)
    hidden_cot = jnp.dot(cotangent, down_bf, preferred_element_type=jnp.float32) * down_scale
    gate_cot = (hidden_cot * upper * sig * (1.0 + gate * (1.0 - sig)) * gate_scale).astype(jnp.bfloat16)
    up_cot = (hidden_cot * act * up_scale).astype(jnp.bfloat16)
    width = FF // N_TP
    gate_bf = gate_weight.astype(jnp.bfloat16)
    up_bf = up_weight.astype(jnp.bfloat16)

    def block_sum(total, index):
        start = (index * width).astype(jnp.int32)
        gc = lax.dynamic_slice_in_dim(gate_cot, start, width, 1)
        uc = lax.dynamic_slice_in_dim(up_cot, start, width, 1)
        gw = lax.dynamic_slice_in_dim(gate_bf, start, width, 1)
        uw = lax.dynamic_slice_in_dim(up_bf, start, width, 1)
        part = jnp.dot(gc, gw.T, preferred_element_type=jnp.float32) + jnp.dot(uc, uw.T, preferred_element_type=jnp.float32)
        return total + part.astype(jnp.bfloat16).astype(jnp.float32), None

    summed, _ = lax.scan(block_sum, jnp.zeros((TOKENS, D), jnp.float32), jnp.arange(N_TP, dtype=jnp.int32))
    input_grad = summed.astype(jnp.bfloat16)
    gate_grad = jnp.dot(inputs.T, gate_cot, preferred_element_type=jnp.float32)
    up_grad = jnp.dot(inputs.T, up_cot, preferred_element_type=jnp.float32)
    down_grad = jnp.dot(cotangent.T, hidden, preferred_element_type=jnp.float32) * down_scale
    return (input_grad, gate_grad, up_grad, down_grad)
```

```python
import jax
import jax.numpy as jnp
from jax import lax
from jax.experimental import pallas as pl
from jax.experimental.pallas import tpu as pltpu
from jax.sharding import PartitionSpec as P

MESH = pl.DeviceIdType.MESH
F32 = jnp.float32
BF16 = jnp.bfloat16
ROWS = 128
HALF = 64
TOK = 512
D = 2048
FFL = 704
GU = 1408
MAIN = 640
NTP = 8


def kernel(
    x_hbm, cot_hbm, gate_hbm, up_hbm, wd_hbm, wgu_hbm, gs_ref, us_ref, ds_ref,
    oi_ref, og_ref, ou_ref, od_ref,
    x, cot, gate, up, hidden, fg, fu, bc,
    wd, wgu, gd, ggu,
    d_r1, d_r2, d_s, d_b1, d_b2, d_f, d_q1, d_q2,
    g_r1, g_r2, g_s, g_b1, g_b2, g_f, g_q1, g_q2,
    tp_out, tp_in,
    local_sem, ag_send, ag_recv, rs_send, rs_recv, tp_send, tp_recv,
):
    rep = lax.axis_index("rep")
    fs = lax.axis_index("fs")
    tp = lax.axis_index("tp")
    y = lax.rem(fs, 4)
    zl = lax.div(fs, 4)
    z = rep * 4 + zl

    def near(dy, dz):
        yy = lax.rem(y + dy + 4, 4)
        zz = lax.rem(z + dz + 8, 8)
        return (lax.div(zz, 4), lax.rem(zz, 4) * 4 + yy, tp)

    def tp_peer(r):
        return (rep, fs, lax.rem(tp + r, NTP))

    def yi(k):
        return lax.rem(y + k + 4, 4)

    def zi(k):
        return lax.rem(zl + k + 4, 4)

    loads = {}
    for k, (src, dst) in enumerate(
        (
            (wd_hbm, wd.at[zl, y]),
            (wgu_hbm, wgu.at[zl, y]),
            (gate_hbm, gate),
            (up_hbm, up),
            (cot_hbm, cot),
            (x_hbm, x),
        )
    ):
        loads[k] = pltpu.make_async_copy(src, dst, local_sem.at[k])
        loads[k].start()

    barrier = pltpu.get_barrier_semaphore()
    peers = [near(1, 0), near(3, 0), near(0, 1), near(0, 7), near(0, 2), near(0, 6)]
    peers += [tp_peer(r) for r in range(1, NTP)]
    for peer in peers:
        pl.semaphore_signal(barrier, inc=1, device_id=peer, device_id_type=MESH)
    loads[0].wait()
    loads[1].wait()
    pl.semaphore_wait(barrier, len(peers))

    sends = []

    def remote(src, dst, send_sem, recv_sem, peer):
        return pltpu.make_async_remote_copy(
            src_ref=src, dst_ref=dst, send_sem=send_sem, recv_sem=recv_sem,
            device_id=peer, device_id_type=MESH,
        )

    AGN = 20

    class Gather:
        def __init__(self, buf, base, first_z):
            self.buf, self.base, self.first_z = buf, base, first_z

        def blk(self, ia, ib):
            if self.first_z:
                return self.buf.at[zi(ia), yi(ib)]
            return self.buf.at[zi(ib), yi(ia)]

        def half(self, ia, ib, h):
            rows = pl.ds(h * HALF, HALF)
            if self.first_z:
                return self.buf.at[zi(ia), yi(ib), rows]
            return self.buf.at[zi(ib), yi(ia), rows]

        def peer_a(self, s):
            return near(0, s) if self.first_z else near(s, 0)

        def peer_b(self, s):
            return near(s, 0) if self.first_z else near(0, s)

        def send(self, k, ref, peer):
            c = remote(ref, ref, ag_send.at[self.base + k], ag_recv.at[self.base + k], peer)
            c.start()
            sends.append(c)

        def got(self, k, ref):
            remote(
                ref, ref, ag_send.at[self.base + k], ag_recv.at[self.base + k], near(1, 0)
            ).wait_recv()

        def own_a(self):
            self.send(0, self.blk(0, 0), self.peer_a(1))
            self.send(1, self.blk(0, 0), self.peer_a(-1))

        def to_b(self, k, ia):
            self.send(k, self.blk(ia, 0), self.peer_b(1))
            self.send(k + 1, self.blk(ia, 0), self.peer_b(-1))

        def own_b(self):
            self.to_b(2, 0)

        def recv_a(self):
            self.got(0, self.blk(-1, 0))
            self.send(4, self.half(-1, 0, 0), self.peer_a(1))
            self.to_b(6, -1)
            self.got(1, self.blk(1, 0))
            self.send(5, self.half(1, 0, 1), self.peer_a(-1))
            self.to_b(8, 1)

        def recv_far(self):
            self.got(4, self.half(2, 0, 0))
            self.got(5, self.half(2, 0, 1))
            self.to_b(10, 2)

        def recv_b(self, n):
            ia = (0, -1, 1, 2)[n]
            k = (2, 6, 8, 10)[n]
            self.got(k, self.blk(ia, -1))
            self.send(12 + 2 * n, self.half(ia, -1, 0), self.peer_b(1))
            self.got(k + 1, self.blk(ia, 1))
            self.send(13 + 2 * n, self.half(ia, 1, 1), self.peer_b(-1))

        def last(self):
            for n in range(4):
                ia = (0, -1, 1, 2)[n]
                self.got(12 + 2 * n, self.half(ia, 2, 0))
                self.got(13 + 2 * n, self.half(ia, 2, 1))

    def add_rows(n, fn):
        @pl.loop(0, n // 16)
        def _(i):
            fn(pl.ds(pl.multiple_of(i * 16, 16), 16))

    class Reduce:
        def __init__(self, grad, r1, r2, s, b1, b2, f, q1, q2, base, first_z):
            self.grad, self.r1, self.r2, self.s = grad, r1, r2, s
            self.b1, self.b2, self.f, self.q1, self.q2 = b1, b2, f, q1, q2
            self.base, self.first_z = base, first_z

        def part(self, ia, h):
            if self.first_z:
                return self.grad.at[zi(ia), pl.ds(2 * h, 2)]
            return self.grad.at[pl.ds(2 * h, 2), yi(ia)]

        def ib(self, k):
            return yi(k) if self.first_z else zi(k)

        def peer_a(self, s):
            return near(0, s) if self.first_z else near(s, 0)

        def peer_b(self, s):
            return near(s, 0) if self.first_z else near(0, s)

        def send(self, k, src, dst, peer):
            c = remote(src, dst, rs_send.at[self.base + k], rs_recv.at[self.base + k], peer)
            c.start()
            sends.append(c)

        def got(self, k, ref):
            remote(
                ref, ref, rs_send.at[self.base + k], rs_recv.at[self.base + k], near(1, 0)
            ).wait_recv()

        def start_far(self, h):
            if h == 0:
                self.send(0, self.part(2, 0), self.r1.at[0], self.peer_a(1))
            else:
                self.send(1, self.part(2, 1), self.r1.at[1], self.peer_a(-1))

        def start_plus(self):
            self.send(2, self.part(1, 1), self.r2.at[0, pl.ds(2, 2)], self.peer_a(1))

        def start_minus(self):
            self.send(3, self.part(-1, 0), self.r2.at[1, pl.ds(0, 2)], self.peer_a(-1))

        def acc_part(self, ia, h, inc):
            for j in range(2):
                def body(rows, j=j):
                    if self.first_z:
                        at = (zi(ia), 2 * h + j, rows)
                    else:
                        at = (2 * h + j, yi(ia), rows)
                    total = self.grad[at].astype(F32) + inc[j, rows].astype(F32)
                    self.grad[at] = total.astype(BF16)

                add_rows(ROWS, body)

        def pass_on(self):
            self.got(0, self.r1.at[0])
            self.acc_part(1, 0, self.r1.at[0])
            self.send(4, self.part(1, 0), self.r2.at[0, pl.ds(0, 2)], self.peer_a(1))
            self.got(1, self.r1.at[1])
            self.acc_part(-1, 1, self.r1.at[1])
            self.send(5, self.part(-1, 1), self.r2.at[1, pl.ds(2, 2)], self.peer_a(-1))

        def gather_own(self):
            self.got(2, self.r2.at[0, pl.ds(2, 2)])
            self.got(3, self.r2.at[1, pl.ds(0, 2)])
            self.got(4, self.r2.at[0, pl.ds(0, 2)])
            self.got(5, self.r2.at[1, pl.ds(2, 2)])
            self.sum_own(2)
            self.send(6, self.s.at[self.ib(2), pl.ds(0, HALF)], self.b1.at[0], self.peer_b(1))
            self.send(7, self.s.at[self.ib(2), pl.ds(HALF, HALF)], self.b1.at[1], self.peer_b(-1))
            self.sum_own(1)
            self.send(
                8, self.s.at[self.ib(1), pl.ds(HALF, HALF)],
                self.b2.at[0, pl.ds(HALF, HALF)], self.peer_b(1),
            )
            self.sum_own(-1)
            self.send(
                9, self.s.at[self.ib(-1), pl.ds(0, HALF)],
                self.b2.at[1, pl.ds(0, HALF)], self.peer_b(-1),
            )
            self.sum_own(0)

        def sum_own(self, k):
            ib = self.ib(k)

            def body(rows):
                at = (zi(0), ib, rows) if self.first_z else (ib, yi(0), rows)
                total = self.grad[at].astype(F32) + self.r2[0, ib, rows].astype(F32)
                total = total + self.r2[1, ib, rows].astype(F32)
                self.s[ib, rows] = total.astype(BF16)

            add_rows(ROWS, body)

        def pass_on_b(self):
            self.got(6, self.b1.at[0])

            def plus(rows):
                total = self.s[self.ib(1), rows].astype(F32) + self.b1[0, rows].astype(F32)
                self.s[self.ib(1), rows] = total.astype(BF16)

            add_rows(HALF, plus)
            self.send(
                10, self.s.at[self.ib(1), pl.ds(0, HALF)],
                self.b2.at[0, pl.ds(0, HALF)], self.peer_b(1),
            )
            self.got(7, self.b1.at[1])

            @pl.loop(0, HALF // 16)
            def _(i):
                low = pl.ds(pl.multiple_of(i * 16, 16), 16)
                rows = pl.ds(pl.multiple_of(HALF + i * 16, 16), 16)
                total = self.s[self.ib(-1), rows].astype(F32) + self.b1[1, low].astype(F32)
                self.s[self.ib(-1), rows] = total.astype(BF16)

            self.send(
                11, self.s.at[self.ib(-1), pl.ds(HALF, HALF)],
                self.b2.at[1, pl.ds(HALF, HALF)], self.peer_b(-1),
            )

        def finish_b(self):
            self.got(8, self.b2.at[0, pl.ds(HALF, HALF)])
            self.got(9, self.b2.at[1, pl.ds(0, HALF)])
            self.got(10, self.b2.at[0, pl.ds(0, HALF)])
            self.got(11, self.b2.at[1, pl.ds(HALF, HALF)])

            def body(rows):
                total = self.s[self.ib(0), rows].astype(F32) + self.b2[0, rows].astype(F32)
                total = total + self.b2[1, rows].astype(F32)
                self.f[rows] = total.astype(BF16)

            add_rows(ROWS, body)
            self.send(12, self.f.at[pl.ds(0, HALF)], self.q1.at[0], near(0, 2))
            self.send(13, self.f.at[pl.ds(HALF, HALF)], self.q1.at[1], near(0, -2))

        def relay(self):
            self.got(12, self.q1.at[0])
            self.send(14, self.q1.at[0], self.q2.at[pl.ds(0, HALF)], near(0, 2))
            self.got(13, self.q1.at[1])
            self.send(15, self.q1.at[1], self.q2.at[pl.ds(HALF, HALF)], near(0, -2))

        def arrive(self):
            self.got(14, self.q2.at[pl.ds(0, HALF)])
            self.got(15, self.q2.at[pl.ds(HALF, HALF)])

    ag_d = Gather(wd, 0, True)
    ag_g = Gather(wgu, AGN, False)
    rs_d = Reduce(gd, d_r1, d_r2, d_s, d_b1, d_b2, d_f, d_q1, d_q2, 0, True)
    rs_g = Reduce(ggu, g_r1, g_r2, g_s, g_b1, g_b2, g_f, g_q1, g_q2, 16, False)

    ag_d.own_a()
    ag_d.own_b()
    ag_g.own_a()
    ag_g.own_b()

    loads[2].wait()
    loads[3].wait()

    @pl.loop(0, TOK // 16)
    def _(i):
        rows = pl.ds(pl.multiple_of(i * 16, 16), 16)
        g = gate[rows, :].astype(F32)
        u = up[rows, :].astype(F32)
        sig = jax.nn.sigmoid(g)
        act = g * sig
        hidden[rows, :] = (act * u).astype(BF16)
        down = ds_ref[...]
        fg[rows, :] = u * sig * (1.0 + g * (1.0 - sig)) * (gs_ref[...] * down)
        fu[rows, :] = act * (us_ref[...] * down)

    ag_d.recv_a()
    ag_g.recv_a()
    ag_d.recv_b(0)
    ag_d.recv_far()
    ag_g.recv_b(0)

    loads[4].wait()

    def down_slab(k):
        zz = zi(k)
        for j in range(2):
            cols = pl.ds(pl.multiple_of(zz * 512 + j * 256, 256), 256)
            out = lax.dot_general(
                cot[:, cols], hidden[...], (((0,), (0,)), ((), ())), preferred_element_type=F32
            ).astype(BF16)
            gd[zz, 2 * j] = out[:ROWS]
            gd[zz, 2 * j + 1] = out[ROWS:]

    @pl.loop(0, 4)
    def _(k):
        zz = k
        for j in range(2):
            cols = pl.ds(pl.multiple_of(zz * 512 + j * 256, 256), 256)
            out = lax.dot_general(
                cot[:, cols], hidden[...], (((0,), (0,)), ((), ())), preferred_element_type=F32
            ).astype(BF16)
            gd[zz, 2 * j] = out[:ROWS]
            gd[zz, 2 * j + 1] = out[ROWS:]

    ag_g.recv_far()
    ag_d.recv_b(1)
    ag_d.recv_b(2)
    ag_g.recv_b(1)
    ag_d.recv_b(3)
    ag_g.recv_b(2)
    ag_d.last()

    @pl.loop(0, 2)
    def _(m):
        rows = pl.ds(pl.multiple_of(m * 256, 256), 256)
        hc = jnp.dot(
            cot[rows, :], wd[...].reshape(D, FFL), preferred_element_type=F32
        )
        gc = (hc * fg[rows, :]).astype(BF16)
        uc = (hc * fu[rows, :]).astype(BF16)
        bc[rows, pl.ds(0, MAIN)] = gc[:, :MAIN]
        bc[rows, pl.ds(MAIN, MAIN)] = uc[:, :MAIN]
        bc[rows, pl.ds(2 * MAIN, 128)] = jnp.concatenate([gc[:, MAIN:], uc[:, MAIN:]], axis=1)

    ag_g.recv_b(3)
    rs_d.start_far(0)
    rs_d.start_far(1)
    rs_d.start_plus()
    rs_d.start_minus()
    loads[5].wait()

    @pl.loop(0, 4)
    def _(k):
        yy = lax.rem(y + 2 + k, 4)
        for j in range(2):
            lo = pl.ds(pl.multiple_of((8 * j + yy) * ROWS, ROWS), ROWS)
            hi = pl.ds(pl.multiple_of((8 * j + 4 + yy) * ROWS, ROWS), ROWS)
            both = jnp.concatenate([x[:, lo], x[:, hi]], axis=1)
            out = lax.dot_general(
                both, bc[...], (((0,), (0,)), ((), ())), preferred_element_type=F32
            ).astype(BF16)
            ggu[2 * j, yy] = out[:ROWS]
            ggu[2 * j + 1, yy] = out[ROWS:]

    rs_g.start_far(0)
    rs_g.start_far(1)
    rs_g.start_plus()
    rs_g.start_minus()

    ag_g.last()

    @pl.loop(0, NTP)
    def _(r):
        t = lax.rem(tp + r, NTP)
        w = wgu[lax.div(t, 2), pl.ds(lax.rem(t, 2) * 2, 2)].reshape(256, GU)
        part = lax.dot_general(
            bc[...], w, (((1,), (1,)), ((), ())), preferred_element_type=F32
        )
        tp_out[r] = part.astype(BF16)

    for r in range(1, NTP):
        c = remote(tp_out.at[r], tp_in.at[r], tp_send.at[r], tp_recv.at[r], tp_peer(r))
        c.start()
        sends.append(c)

    rs_d.pass_on()
    rs_g.pass_on()
    rs_d.gather_own()
    rs_d.pass_on_b()
    rs_d.finish_b()
    rs_d.relay()
    rs_g.gather_own()
    rs_g.pass_on_b()
    rs_g.finish_b()
    rs_d.arrive()

    def down_out(rows):
        total = d_f[rows].astype(F32) + d_q2[rows].astype(F32)
        od_ref[rows, :] = total * ds_ref[...]

    add_rows(ROWS, down_out)

    for r in range(1, NTP):
        remote(
            tp_in.at[r], tp_in.at[r], tp_send.at[r], tp_recv.at[r], tp_peer(r)
        ).wait_recv()

    def input_out(rows):
        total = tp_out[0, rows].astype(F32)
        for r in range(1, NTP):
            total = total + tp_in[r, rows].astype(F32)
        oi_ref[rows, :] = total.astype(BF16)

    add_rows(TOK, input_out)

    rs_g.relay()
    rs_g.arrive()

    def gate_up_out(rows):
        total = g_f[rows].astype(F32) + g_q2[rows].astype(F32)
        og_ref[rows, pl.ds(0, MAIN)] = total[:, :MAIN]
        ou_ref[rows, pl.ds(0, MAIN)] = total[:, MAIN : 2 * MAIN]
        og_ref[rows, pl.ds(MAIN, HALF)] = total[:, 2 * MAIN : 2 * MAIN + HALF]
        ou_ref[rows, pl.ds(MAIN, HALF)] = total[:, 2 * MAIN + HALF :]

    add_rows(ROWS, gate_up_out)

    for c in sends:
        c.wait_send()


def reduce_scratch(c):
    return [
        pltpu.VMEM((2, 2, ROWS, c), BF16),
        pltpu.VMEM((2, 4, ROWS, c), BF16),
        pltpu.VMEM((4, ROWS, c), BF16),
        pltpu.VMEM((2, HALF, c), BF16),
        pltpu.VMEM((2, ROWS, c), BF16),
        pltpu.VMEM((ROWS, c), BF16),
        pltpu.VMEM((2, HALF, c), BF16),
        pltpu.VMEM((ROWS, c), BF16),
    ]


def local(
    inputs, cotangent, gate_pre, up_pre, gate_weight, up_weight, down_weight,
    gate_scale, up_scale, down_scale,
):
    wd = down_weight.astype(BF16)
    wgu = jnp.concatenate(
        [gate_weight[:, :MAIN], up_weight[:, :MAIN], gate_weight[:, MAIN:], up_weight[:, MAIN:]],
        axis=1,
    ).astype(BF16)
    hbm = pl.BlockSpec(memory_space=pl.ANY)
    vmem = pl.BlockSpec(memory_space=pltpu.VMEM)
    return pl.pallas_call(
        kernel,
        out_shape=(
            jax.ShapeDtypeStruct((TOK, 256), BF16),
            jax.ShapeDtypeStruct((ROWS, FFL), F32),
            jax.ShapeDtypeStruct((ROWS, FFL), F32),
            jax.ShapeDtypeStruct((ROWS, FFL), F32),
        ),
        in_specs=[hbm] * 6 + [vmem] * 3,
        out_specs=(vmem,) * 4,
        scratch_shapes=[
            pltpu.VMEM((TOK, D), BF16),
            pltpu.VMEM((TOK, D), BF16),
            pltpu.VMEM((TOK, FFL), BF16),
            pltpu.VMEM((TOK, FFL), BF16),
            pltpu.VMEM((TOK, FFL), BF16),
            pltpu.VMEM((TOK, FFL), F32),
            pltpu.VMEM((TOK, FFL), F32),
            pltpu.VMEM((TOK, GU), BF16),
            pltpu.VMEM((4, 4, ROWS, FFL), BF16),
            pltpu.VMEM((4, 4, ROWS, GU), BF16),
            pltpu.VMEM((4, 4, ROWS, FFL), BF16),
            pltpu.VMEM((4, 4, ROWS, GU), BF16),
            *reduce_scratch(FFL),
            *reduce_scratch(GU),
            pltpu.VMEM((NTP, TOK, 256), BF16),
            pltpu.VMEM((NTP, TOK, 256), BF16),
            pltpu.SemaphoreType.DMA((6,)),
            pltpu.SemaphoreType.DMA((40,)),
            pltpu.SemaphoreType.DMA((40,)),
            pltpu.SemaphoreType.DMA((32,)),
            pltpu.SemaphoreType.DMA((32,)),
            pltpu.SemaphoreType.DMA((NTP,)),
            pltpu.SemaphoreType.DMA((NTP,)),
        ],
        compiler_params=pltpu.CompilerParams(
            collective_id=0, has_side_effects=True, vmem_limit_bytes=60 * 1024 * 1024
        ),
    )(inputs, cotangent, gate_pre, up_pre, wd, wgu, gate_scale, up_scale, down_scale)


def solution(mesh):
    rows = ("rep", "fs")
    in_specs = (
        P(rows, None), P(rows, None), P(rows, "tp"), P(rows, "tp"),
        P("fs", "tp"), P("fs", "tp"), P("fs", "tp"),
        P(None, "tp"), P(None, "tp"), P(None, "tp"),
    )
    out_specs = (P(rows, "tp"), P("fs", "tp"), P("fs", "tp"), P("fs", "tp"))
    return jax.shard_map(local, mesh=mesh, in_specs=in_specs, out_specs=out_specs, check_vma=False)
```

```python
import jax
import jax.numpy as jnp
from jax import lax
from jax.experimental import pallas as pl
from jax.experimental.pallas import tpu as pltpu
from jax.sharding import PartitionSpec as P

MESH = pl.DeviceIdType.MESH
F32 = jnp.float32
BF16 = jnp.bfloat16
LANES = 128
TOK = 512
D = 2048
FFL = 704
GU = 2 * FFL
ALL = 3 * FFL
NTP = 8

PIECES = (
    ("d", 0, 704, True, True),
    ("g", 704, 704, False, False),
    ("u", 1408, 704, True, True),
)
ORDER = (
    "ag0 g", "ag0 d", "ew", "a1 g", "b0+ g", "b0- g", "a0 g", "a1 d", "b0- d", "b0+ d", "a0 d",
    "far g", "b2+ g", "b2- g", "b2+ d", "b2- d", "ag0 u", "b1- g", "b1+ g", "far d", "b1+ d",
    "b1- d", "b3+ g", "b3- g", "b0- u", "b0+ u", "a1 u", "a0 u", "b3+ d", "b3- d", "down",
    "rs0 d", "last g", "far u", "b2+ u", "b2- u", "b1- u", "b1+ u", "p0 d", "last d", "p1 d",
    "hc", "b3+ u", "b3- u", "gu", "rs0 u", "rs0 g", "last u", "part", "p1 g", "p0 g", "p0 u",
    "p1 u", "own d", "own g", "q1 d", "q0 d", "own u", "q0 g", "q1 g", "fin d", "q1 u", "q0 u",
    "fin g", "fin u", "y0 d", "y1 d", "tp", "y0 g", "y1 g", "y0 u", "y1 u", "arr d", "arr g",
    "arr u",
)

def kernel(
    x_hbm, cot_hbm, gate_hbm, up_hbm, wd_hbm, wg_hbm, wu_hbm, gs_ref, us_ref, ds_ref,
    oi_ref, og_ref, ou_ref, od_ref,
    x, cot, gate, up, w32, scales, hidden, fg, fu, bc,
    w, grad, r1, r2, own, b1, b2, final, q1, q2,
    tp_out, tp_in,
    local_sem, ag_send, ag_recv, rs_send, rs_recv, tp_send, tp_recv,
):
    rep = lax.axis_index("rep")
    fs = lax.axis_index("fs")
    tp = lax.axis_index("tp")
    y = lax.rem(fs, 4)
    zl = lax.div(fs, 4)
    z = rep * 4 + zl

    def near(dy, dz):
        yy = lax.rem(y + dy + 4, 4)
        zz = lax.rem(z + dz + 8, 8)
        return (lax.div(zz, 4), lax.rem(zz, 4) * 4 + yy, tp)

    def tp_peer(r):
        return (rep, fs, lax.rem(tp + r, NTP))

    def yi(k):
        return lax.rem(y + k + 4, 4)

    def zi(k):
        return lax.rem(zl + k + 4, 4)

    def chunks(n, fn):
        @pl.loop(0, n // 32)
        def _(i):
            fn(i * 32)

    def rows32(start):
        return pl.ds(pl.multiple_of(start, 16), 32)

    loads = []
    for k, (src, dst) in enumerate(
        (
            (wd_hbm, w32.at[pl.ds(0, FFL)]),
            (wg_hbm, w32.at[pl.ds(FFL, FFL)]),
            (wu_hbm, w32.at[pl.ds(GU, FFL)]),
            (gate_hbm, gate),
            (up_hbm, up),
            (cot_hbm, cot),
            (x_hbm, x),
        )
    ):
        loads.append(pltpu.make_async_copy(src, dst, local_sem.at[k]))
        loads[k].start()

    barrier = pltpu.get_barrier_semaphore()
    peers = [near(1, 0), near(3, 0), near(0, 1), near(0, 7), near(0, 2), near(0, 6)]
    peers += [tp_peer(r) for r in range(1, NTP)]
    for peer in peers:
        pl.semaphore_signal(barrier, inc=1, device_id=peer, device_id_type=MESH)

    for k in range(3):
        loads[k].wait()

    def narrow(i):
        w[zl, y, rows32(i)] = w32[rows32(i)].astype(BF16)

    chunks(ALL, narrow)
    pl.semaphore_wait(barrier, len(peers))

    sends = []

    def remote(src, dst, send_sem, recv_sem, peer):
        return pltpu.make_async_remote_copy(
            src_ref=src, dst_ref=dst, send_sem=send_sem, recv_sem=recv_sem,
            device_id=peer, device_id_type=MESH,
        )

    class Gather:
        def __init__(self, base, lo, n, first_z):
            self.base, self.lo, self.n, self.first_z = base, lo, n, first_z

        def at(self, ia, ib, rows):
            if self.first_z:
                return w.at[zi(ia), yi(ib), rows]
            return w.at[zi(ib), yi(ia), rows]

        def blk(self, ia, ib):
            return self.at(ia, ib, pl.ds(self.lo, self.n))

        def half(self, ia, ib, h):
            return self.at(ia, ib, pl.ds(self.lo + h * (self.n // 2), self.n // 2))

        def peer_a(self, s):
            return near(0, s) if self.first_z else near(s, 0)

        def peer_b(self, s):
            return near(s, 0) if self.first_z else near(0, s)

        def send(self, k, ref, peer):
            k += self.base
            c = remote(ref, ref, ag_send.at[k], ag_recv.at[k], peer)
            c.start()
            sends.append(c)

        def got(self, k, ref):
            k += self.base
            remote(ref, ref, ag_send.at[k], ag_recv.at[k], near(1, 0)).wait_recv()

        def to_b(self, k, ia):
            self.send(k, self.blk(ia, 0), self.peer_b(1))
            self.send(k + 1, self.blk(ia, 0), self.peer_b(-1))

        def step(self, name):
            if name == "ag0":
                self.send(0, self.blk(0, 0), self.peer_a(1))
                self.send(1, self.blk(0, 0), self.peer_a(-1))
                self.to_b(2, 0)
            elif name == "a0":
                self.got(0, self.blk(-1, 0))
                self.send(4, self.half(-1, 0, 0), self.peer_a(1))
                self.to_b(6, -1)
            elif name == "a1":
                self.got(1, self.blk(1, 0))
                self.send(5, self.half(1, 0, 1), self.peer_a(-1))
                self.to_b(8, 1)
            elif name == "far":
                self.got(4, self.half(2, 0, 0))
                self.got(5, self.half(2, 0, 1))
                self.to_b(10, 2)
            elif name == "last":
                for n in range(4):
                    ia = (0, -1, 1, 2)[n]
                    self.got(12 + 2 * n, self.half(ia, 2, 0))
                    self.got(13 + 2 * n, self.half(ia, 2, 1))
            elif name[0] == "b":
                n = int(name[1])
                ia, k = (0, -1, 1, 2)[n], (2, 6, 8, 10)[n]
                if name[2] == "+":
                    self.got(k, self.blk(ia, -1))
                    self.send(12 + 2 * n, self.half(ia, -1, 0), self.peer_b(1))
                else:
                    self.got(k + 1, self.blk(ia, 1))
                    self.send(13 + 2 * n, self.half(ia, 1, 1), self.peer_b(-1))
            else:
                return False
            return True

    class Reduce:
        def __init__(self, base, lo, n, first_z):
            self.base, self.lo, self.n, self.first_z = base, lo, n, first_z
            h = n // 2
            self.rows = pl.ds(lo, n)
            self.half = (pl.ds(lo, h), pl.ds(lo + h, h))
            self.small = pl.ds(lo // 2, h)

        def part(self, ia, h):
            if self.first_z:
                return grad.at[zi(ia), pl.ds(2 * h, 2), self.rows]
            return grad.at[pl.ds(2 * h, 2), yi(ia), self.rows]

        def ib(self, k):
            return yi(k) if self.first_z else zi(k)

        def peer_a(self, s):
            return near(0, s) if self.first_z else near(s, 0)

        def peer_b(self, s):
            return near(s, 0) if self.first_z else near(0, s)

        def send(self, k, src, dst, peer):
            k += self.base
            c = remote(src, dst, rs_send.at[k], rs_recv.at[k], peer)
            c.start()
            sends.append(c)

        def got(self, k, ref):
            k += self.base
            remote(ref, ref, rs_send.at[k], rs_recv.at[k], near(1, 0)).wait_recv()

        def far(self, s, h):
            return r1.at[h, pl.ds(0, 2), self.rows]

        def near_part(self, s, h):
            return r2.at[s, pl.ds(2 * h, 2), self.rows]

        def add_part(self, ia, h):
            for j in range(2):
                def body(i, j=j):
                    rows = rows32(self.lo + i)
                    at = (zi(ia), 2 * h + j, rows) if self.first_z else (2 * h + j, yi(ia), rows)
                    total = grad[at].astype(F32) + r1[h, j, rows].astype(F32)
                    grad[at] = total.astype(BF16)

                chunks(self.n, body)

        def sum_own(self, k):
            ib = self.ib(k)

            def body(i):
                rows = rows32(self.lo + i)
                at = (zi(0), ib, rows) if self.first_z else (ib, yi(0), rows)
                total = grad[at].astype(F32) + r2[0, ib, rows].astype(F32)
                total = total + r2[1, ib, rows].astype(F32)
                own[ib, rows] = total.astype(BF16)

            chunks(self.n, body)

        def add_half(self, k, h):
            ib = self.ib(k)

            def body(i):
                rows = rows32(self.lo + h * (self.n // 2) + i)
                total = own[ib, rows].astype(F32) + b1[h, rows32(self.lo // 2 + i)].astype(F32)
                own[ib, rows] = total.astype(BF16)

            chunks(self.n // 2, body)

        def step(self, name):
            if name == "rs0":
                self.send(0, self.part(2, 0), self.far(0, 0), self.peer_a(1))
                self.send(1, self.part(2, 1), self.far(1, 1), self.peer_a(-1))
                self.send(2, self.part(1, 1), self.near_part(0, 1), self.peer_a(1))
                self.send(3, self.part(-1, 0), self.near_part(1, 0), self.peer_a(-1))
            elif name == "p0":
                self.got(0, self.far(0, 0))
                self.add_part(1, 0)
                self.send(4, self.part(1, 0), self.near_part(0, 0), self.peer_a(1))
            elif name == "p1":
                self.got(1, self.far(1, 1))
                self.add_part(-1, 1)
                self.send(5, self.part(-1, 1), self.near_part(1, 1), self.peer_a(-1))
            elif name == "own":
                self.got(2, self.near_part(0, 1))
                self.got(3, self.near_part(1, 0))
                self.got(4, self.near_part(0, 0))
                self.got(5, self.near_part(1, 1))
                lo, hi = self.half
                self.sum_own(2)
                self.send(6, own.at[self.ib(2), lo], b1.at[0, self.small], self.peer_b(1))
                self.send(7, own.at[self.ib(2), hi], b1.at[1, self.small], self.peer_b(-1))
                self.sum_own(1)
                self.send(8, own.at[self.ib(1), hi], b2.at[0, hi], self.peer_b(1))
                self.sum_own(-1)
                self.send(9, own.at[self.ib(-1), lo], b2.at[1, lo], self.peer_b(-1))
                self.sum_own(0)
            elif name == "q0":
                lo = self.half[0]
                self.got(6, b1.at[0, self.small])
                self.add_half(1, 0)
                self.send(10, own.at[self.ib(1), lo], b2.at[0, lo], self.peer_b(1))
            elif name == "q1":
                hi = self.half[1]
                self.got(7, b1.at[1, self.small])
                self.add_half(-1, 1)
                self.send(11, own.at[self.ib(-1), hi], b2.at[1, hi], self.peer_b(-1))
            elif name == "fin":
                lo, hi = self.half
                self.got(8, b2.at[0, hi])
                self.got(9, b2.at[1, lo])
                self.got(10, b2.at[0, lo])
                self.got(11, b2.at[1, hi])
                ib = self.ib(0)

                def body(i):
                    rows = rows32(self.lo + i)
                    total = own[ib, rows].astype(F32) + b2[0, rows].astype(F32)
                    total = total + b2[1, rows].astype(F32)
                    final[rows] = total.astype(BF16)

                chunks(self.n, body)
                self.send(12, final.at[lo], q1.at[0, self.small], near(0, 2))
                self.send(13, final.at[hi], q1.at[1, self.small], near(0, -2))
            elif name == "y0":
                self.got(12, q1.at[0, self.small])
                self.send(14, q1.at[0, self.small], q2.at[self.half[0]], near(0, 2))
            elif name == "y1":
                self.got(13, q1.at[1, self.small])
                self.send(15, q1.at[1, self.small], q2.at[self.half[1]], near(0, -2))
            elif name == "arr":
                self.got(14, q2.at[self.half[0]])
                self.got(15, q2.at[self.half[1]])
                which = self.lo // FFL
                out_ref = (od_ref, og_ref, ou_ref)[which]

                def out(i):
                    rows = rows32(self.lo + i)
                    total = final[rows].astype(F32) + q2[rows].astype(F32)
                    to = rows32(self.lo - which * FFL + i)
                    if which == 0:
                        total = total * scales[2, to]
                    out_ref[to, :] = total

                chunks(self.n, out)
            else:
                return False
            return True

    def elementwise():
        for k, ref in enumerate((gs_ref, us_ref, ds_ref)):
            scales[k] = jnp.broadcast_to(ref[...], (LANES, FFL)).T
        loads[3].wait()
        loads[4].wait()

        def body(i):
            rows = rows32(i)
            g = gate[rows, :].astype(F32)
            u = up[rows, :].astype(F32)
            sig = jax.nn.sigmoid(g)
            act = g * sig
            hidden[rows, :] = (act * u).astype(BF16)
            down = scales[2, rows]
            gs = jnp.concatenate([scales[0, rows] * down] * 4, axis=1)
            us = jnp.concatenate([scales[1, rows] * down] * 4, axis=1)
            fg[rows, :] = u * sig * (1.0 + g * (1.0 - sig)) * gs
            fu[rows, :] = act * us

        chunks(FFL, body)

    def down_grads():
        loads[5].wait()

        @pl.loop(0, 8)
        def _(k):
            zz, yy = lax.div(k, 2), lax.rem(k, 2) * 2
            cols = pl.ds(pl.multiple_of(k * 256, 256), 256)
            out = jnp.dot(hidden[...], cot[:, cols], preferred_element_type=F32).astype(BF16)
            grad[zz, yy, pl.ds(0, FFL)] = out[:, :LANES]
            grad[zz, yy + 1, pl.ds(0, FFL)] = out[:, LANES:]

    def cotangents():
        @pl.loop(0, 2)
        def _(m):
            cols = pl.ds(pl.multiple_of(m * 256, 256), 256)
            whole = jnp.concatenate(
                [w[i // 4, i % 4, pl.ds(0, FFL)] for i in range(16)], axis=1
            )
            hc = lax.dot_general(
                whole, cot[cols, :], (((1,), (1,)), ((), ())), preferred_element_type=F32
            )
            bc[pl.ds(0, FFL), cols] = (hc * fg[:, cols]).astype(BF16)
            bc[pl.ds(FFL, FFL), cols] = (hc * fu[:, cols]).astype(BF16)

    def gate_up_grads():
        loads[6].wait()

        @pl.loop(0, 8)
        def _(k):
            zz, yy = lax.div(k, 2), lax.rem(k, 2) * 2
            cols = pl.ds(pl.multiple_of(k * 256, 256), 256)
            out = jnp.dot(bc[...], x[:, cols], preferred_element_type=F32).astype(BF16)
            grad[zz, yy, pl.ds(FFL, GU)] = out[:, :LANES]
            grad[zz, yy + 1, pl.ds(FFL, GU)] = out[:, LANES:]

    def partial_inputs():
        @pl.loop(0, NTP)
        def _(r):
            t = lax.rem(tp + r, NTP)
            zz, yy = lax.div(t, 2), lax.rem(t, 2) * 2
            rows = pl.ds(FFL, GU)
            both = jnp.concatenate([w[zz, yy, rows], w[zz, yy + 1, rows]], axis=1)
            part = lax.dot_general(
                bc[...], both, (((0,), (0,)), ((), ())), preferred_element_type=F32
            )
            tp_out[r] = part.astype(BF16)

        for r in range(1, NTP):
            c = remote(tp_out.at[r], tp_in.at[r], tp_send.at[r], tp_recv.at[r], tp_peer(r))
            c.start()
            sends.append(c)

    def input_grad():
        for r in range(1, NTP):
            remote(
                tp_in.at[r], tp_in.at[r], tp_send.at[r], tp_recv.at[r], tp_peer(r)
            ).wait_recv()

        def body(i):
            rows = rows32(i)
            total = tp_out[0, rows].astype(F32)
            for r in range(1, NTP):
                total = total + tp_in[r, rows].astype(F32)
            oi_ref[rows, :] = total.astype(BF16)

        chunks(TOK, body)

    gathers = {}
    reduces = {}
    for i, (name, lo, n, ag_z, rs_z) in enumerate(PIECES):
        gathers[name] = Gather(20 * i, lo, n, ag_z)
        reduces[name] = Reduce(16 * i, lo, n, rs_z)
    work = {
        "ew": elementwise, "down": down_grads, "hc": cotangents,
        "gu": gate_up_grads, "part": partial_inputs, "tp": input_grad,
    }
    for step in ORDER:
        name, *piece = step.split(" ")
        if not piece:
            work[name]()
        elif not gathers[piece[0]].step(name):
            assert reduces[piece[0]].step(name)

    for c in sends:
        c.wait_send()


def local(
    inputs, cotangent, gate_pre, up_pre, gate_weight, up_weight, down_weight,
    gate_scale, up_scale, down_scale,
):
    hbm = pl.BlockSpec(memory_space=pl.ANY)
    vmem = pl.BlockSpec(memory_space=pltpu.VMEM)
    sem = pltpu.SemaphoreType.DMA
    half = ALL // 2
    oi, og, ou, od = pl.pallas_call(
        kernel,
        out_shape=(
            jax.ShapeDtypeStruct((TOK, 256), BF16),
            jax.ShapeDtypeStruct((FFL, LANES), F32),
            jax.ShapeDtypeStruct((FFL, LANES), F32),
            jax.ShapeDtypeStruct((FFL, LANES), F32),
        ),
        in_specs=[hbm] * 7 + [vmem] * 3,
        out_specs=(vmem,) * 4,
        scratch_shapes=[
            pltpu.VMEM((TOK, D), BF16),
            pltpu.VMEM((TOK, D), BF16),
            pltpu.VMEM((FFL, TOK), BF16),
            pltpu.VMEM((FFL, TOK), BF16),
            pltpu.VMEM((ALL, LANES), F32),
            pltpu.VMEM((3, FFL, LANES), F32),
            pltpu.VMEM((FFL, TOK), BF16),
            pltpu.VMEM((FFL, TOK), F32),
            pltpu.VMEM((FFL, TOK), F32),
            pltpu.VMEM((GU, TOK), BF16),
            pltpu.VMEM((4, 4, ALL, LANES), BF16),
            pltpu.VMEM((4, 4, ALL, LANES), BF16),
            pltpu.VMEM((2, 2, ALL, LANES), BF16),
            pltpu.VMEM((2, 4, ALL, LANES), BF16),
            pltpu.VMEM((4, ALL, LANES), BF16),
            pltpu.VMEM((2, half, LANES), BF16),
            pltpu.VMEM((2, ALL, LANES), BF16),
            pltpu.VMEM((ALL, LANES), BF16),
            pltpu.VMEM((2, half, LANES), BF16),
            pltpu.VMEM((ALL, LANES), BF16),
            pltpu.VMEM((NTP, TOK, 256), BF16),
            pltpu.VMEM((NTP, TOK, 256), BF16),
            sem((7,)),
            sem((20 * len(PIECES),)),
            sem((20 * len(PIECES),)),
            sem((16 * len(PIECES),)),
            sem((16 * len(PIECES),)),
            sem((NTP,)),
            sem((NTP,)),
        ],
        compiler_params=pltpu.CompilerParams(
            collective_id=0, has_side_effects=True, vmem_limit_bytes=58 * 1024 * 1024
        ),
    )(
        inputs, cotangent, gate_pre.T, up_pre.T,
        down_weight.T, gate_weight.T, up_weight.T, gate_scale, up_scale, down_scale,
    )
    return oi, og.T, ou.T, od.T


def solution(mesh):
    rows = ("rep", "fs")
    in_specs = (
        P(rows, None), P(rows, None), P(rows, "tp"), P(rows, "tp"),
        P("fs", "tp"), P("fs", "tp"), P("fs", "tp"),
        P(None, "tp"), P(None, "tp"), P(None, "tp"),
    )
    out_specs = (P(rows, "tp"), P("fs", "tp"), P("fs", "tp"), P("fs", "tp"))
    return jax.shard_map(local, mesh=mesh, in_specs=in_specs, out_specs=out_specs, check_vma=False)
```

```python
import jax
import jax.numpy as jnp
from jax import lax
from jax.experimental import pallas as pl
from jax.experimental.pallas import tpu as pltpu
from jax.sharding import PartitionSpec as P

MESH = pl.DeviceIdType.MESH
F32 = jnp.float32
BF16 = jnp.bfloat16
LANES = 128
TOK = 512
HT = TOK // 2
D = 2048
QD = D // 4
FFL = 704
GU = 2 * FFL
ALL = 3 * FFL
H = FFL // 2
Q = FFL // 4
SIDES = (0, -1, 1, 2)

ORDER = (
    "st 1", "st 0", "ys 0 0", "ys 1 0", "ys 1 1", "ys 1 2", "yr 0 0 -1", "ys 1 3", "sc",
    "ys 0 3", "ys 0 1", "st 2", "c0", "ys 2 3", "sgu", "ys 0 2", "ys 2 2", "yr 0 1 -1",
    "yr 1 3 1", "c1", "ys 2 0", "yr 2 3 -1", "sx", "ys 2 1", "ew", "yr 1 1 -1", "yr 2 2 1",
    "yr 2 0 1", "yr 0 3 -1", "c2", "yr 1 3 -1", "yr 0 2 1", "yr 1 2 1", "yr 0 1 1",
    "yr 0 2 -1", "yr 2 2 -1", "yr 0 3 1", "down", "x0", "yr 2 0 -1", "yr 0 0 1", "yr 1 0 1",
    "yt 0 -1", "yr 2 1 1", "yr 2 1 -1", "ps 0", "yr 2 3 1", "rs 0", "yt 2 1", "yr 1 2 -1",
    "yt 2 -1", "yf 0", "yt 0 1", "last 0", "x1", "hc", "x2", "r+ 0", "r- 0", "gu 2", "yf 2",
    "yr 1 1 1", "ps 2", "yr 1 0 -1", "rs 2", "own 0", "gu 1", "ps 1", "yf 1", "yt 1 1",
    "yt 1 -1", "r- 2", "r+ 2", "fin 0", "rs 1", "own 2", "last 1", "last 2", "y 0 1", "y 0 0",
    "part", "r+ 1", "r- 1", "fin 2", "own 1", "y 2 0", "p 0", "p 1", "y 2 1", "fin 1", "arr 0",
    "psum", "y 1 1", "arr 2", "y 1 0", "tp", "arr 1",
)

def kernel(
    x_hbm, cot_hbm, gate_hbm, up_hbm, wd_hbm, wg_hbm, wu_hbm, gs_ref, us_ref, ds_ref,
    oi_ref, og_ref, ou_ref, od_ref,
    x, cot, gate, up, w32, scales, down_col, hidden, fg, fu, bc,
    w, mine, grad, sib, r1, r2, own, zr, zs, final, q1, q2,
    tp_out, xr1, xr2, from_home, from_guest,
    local_sem, send_sem, recv_sem,
):
    rep = lax.axis_index("rep")
    fs = lax.axis_index("fs")
    tp = lax.axis_index("tp")
    y = lax.rem(fs, 4)
    zl = lax.div(fs, 4)
    z = rep * 4 + zl
    xx = lax.div(tp, 2)
    h = lax.rem(tp, 2)
    p = lax.rem(zl, 2)
    home = h == p
    guest = h != p

    def dev(dx, dy, dz, core):
        nx = lax.rem(xx + dx + 4, 4)
        ny = lax.rem(y + dy + 4, 4)
        nz = lax.rem(z + dz + 8, 8)
        return (lax.div(nz, 4), lax.rem(nz, 4) * 4 + ny, nx * 2 + core)

    def yi(k):
        return lax.rem(y + k + 4, 4)

    def zi(k):
        return lax.rem(zl + k + 4, 4)

    def chunks(n, size, fn):
        if n == size:
            fn(0, size)
            return

        @pl.loop(0, n // size)
        def _(i):
            fn(i * size, size)

    def span(start, size):
        return pl.ds(start if isinstance(start, int) else pl.multiple_of(start, 16), size)

    def half(i, k):
        return pl.ds(pl.multiple_of(i * FFL + k * H, 16), H)

    def quarter(i, k, q):
        return pl.ds(pl.multiple_of(i * FFL + k * H + q * Q, 16), Q)

    def small(i):
        return pl.ds(i * H, H)

    send_ids, recv_ids = {}, {}
    sends = []

    def remote(src, dst, s, r, peer):
        return pltpu.make_async_remote_copy(
            src_ref=src, dst_ref=dst, send_sem=send_sem.at[s], recv_sem=recv_sem.at[r],
            device_id=peer, device_id_type=MESH,
        )

    def rid(name, spread):
        key = name if spread is None else (*name, "by")
        if key not in recv_ids:
            recv_ids[key] = sum(recv_sizes)
            recv_sizes.append(1 if spread is None else 2)
        return recv_ids[key] if spread is None else recv_ids[key] + spread

    recv_sizes = []

    def send(name, src, dst, peer, tag="", by=None):
        s = send_ids.setdefault((*name, tag), len(send_ids))
        remote(src, dst, s, rid(name, by), peer).start()
        sends.append((None, lambda: (src, dst, peer), s))

    def send_if(cond, name, make, tag=""):
        s = send_ids.setdefault((*name, tag), len(send_ids))
        src, dst, peer = make()
        remote(src, dst, s, rid(name, None), peer).start()
        sends.append((cond, make, s))

    def got(name, dst, by=None):
        remote(dst, dst, 0, rid(name, by), dev(0, 1, 0, h)).wait_recv()

    loads = []
    for k, (src, dst) in enumerate(
        (
            (wd_hbm, w32.at[pl.ds(0, FFL)]),
            (wg_hbm, w32.at[pl.ds(FFL, FFL)]),
            (wu_hbm, w32.at[pl.ds(GU, FFL)]),
            (gate_hbm, gate),
            (up_hbm, up),
            (cot_hbm, cot),
            (x_hbm, x),
        )
    ):
        loads.append(pltpu.make_async_copy(src, dst, local_sem.at[k]))
    for k in range(3):
        loads[k].start()

    barrier = pltpu.get_barrier_semaphore()
    peers = [dev(0, 1, 0, h), dev(0, -1, 0, h), dev(1, 0, 0, h), dev(-1, 0, 0, h)]
    for core in range(2):
        peers += [dev(0, 0, k, core) for k in (1, -1, 2, -2)]
    peers.append(dev(0, 0, 0, 1 - h))
    for peer in peers:
        pl.semaphore_signal(barrier, inc=1, device_id=peer, device_id_type=MESH)

    @pl.when(home)
    def _():
        for k in range(3, 7):
            loads[k].start()

    for k in range(3):
        loads[k].wait()

    @pl.when(home)
    def _():
        def narrow(i, n):
            w[zl, y, span(i, n)] = w32[span(i, n)].astype(BF16)

        chunks(ALL, Q, narrow)

    @pl.when(guest)
    def _():
        def narrow(i, n):
            mine[span(i, n)] = w32[span(i, n)].astype(BF16)

        chunks(ALL, Q, narrow)

    pl.semaphore_wait(barrier, len(peers))

    def other(core):
        return dev(0, 0, 0, core)

    def start(i):
        whole = pl.ds(i * FFL, FFL)

        @pl.when(home)
        def _():
            send_if(
                True, (i, "own"),
                lambda: (w.at[zl, y, whole], w.at[zl, y, whole], other(1 - h)),
            )
            for k in range(2):
                for q, s in ((0, 2), (1, -2)):
                    def make(k=k, q=q, s=s):
                        ref = w.at[zl, y, quarter(i, k, q)]
                        return ref, ref, dev(0, 0, s, k)

                    send_if(True, (i, "zq", q), make, k)

        @pl.when(guest)
        def _():
            for k in range(2):
                for s in (1, -1):
                    def make(k=k, s=s):
                        rows = half(i, k)
                        return mine.at[rows], w.at[zl, y, rows], dev(0, 0, s, k)

                    send_if(False, (i, "z", s), make, k)

    def swap(src, dst, name, wide):
        @pl.when(guest)
        def _():
            for s, part in ((1, pl.ds(0, HT)), (-1, pl.ds(HT, HT))):
                def make(s=s, part=part):
                    at = (part, qcols(0)) if wide else (slice(None), part)
                    return src.at[at], dst.at[at], dev(0, 0, s, p)

                send_if(False, (name, s), make)

    def swapped(dst, name, wide):
        for s, part in ((1, pl.ds(0, HT)), (-1, pl.ds(HT, HT))):
            at = (part, qcols(0)) if wide else (slice(None), part)
            got((name, s), dst.at[at])

    def qcols(k):
        return pl.ds(pl.multiple_of(lax.rem(xx + k + 4, 4) * QD, QD), QD)

    def spread0(dst, name):
        @pl.when(guest)
        def _():
            swapped(dst, name, True)
            for s in (1, -1):
                def make(s=s):
                    ref = dst.at[:, qcols(0)]
                    return ref, ref, dev(s, 0, 0, h)

                send_if(False, (name, "x", s), make)

    def spread1(dst, name):
        @pl.when(guest)
        def _():
            for s, part in ((1, pl.ds(0, HT)), (-1, pl.ds(HT, HT))):
                got((name, "x", s), dst.at[:, qcols(-s)])

                def make(s=s, part=part):
                    ref = dst.at[part, qcols(-s)]
                    return ref, ref, dev(s, 0, 0, h)

                send_if(False, (name, "xf", s), make)

    def spread2(dst, name, load):
        @pl.when(guest)
        def _():
            for s, part in ((1, pl.ds(0, HT)), (-1, pl.ds(HT, HT))):
                got((name, "xf", s), dst.at[part, qcols(2)])

        @pl.when(home)
        def _():
            loads[load].wait()

    def ys(i, c):
        ref = w.at[zi(SIDES[c]), y, half(i, h)]
        if c == 0:
            @pl.when(guest)
            def _():
                whole = pl.ds(i * FFL, FFL)
                got((i, "own"), w.at[zl, y, whole])
        elif c < 3:
            got((i, "z", -SIDES[c]), ref)
        else:
            for q in range(2):
                got((i, "zq", q), w.at[zi(2), y, quarter(i, h, q)])
        for s in (1, -1):
            send((i, "y", c, s), ref, ref, dev(0, s, 0, h))
        if c:
            send((i, "s", c), ref, ref, other(1 - h))

    def yr(i, c, s):
        got((i, "y", c, s), w.at[zi(SIDES[c]), yi(-s), half(i, h)])
        q = 0 if s == 1 else 1
        ref = w.at[zi(SIDES[c]), yi(-s), quarter(i, h, q)]
        send((i, "f", c, s), ref, ref, dev(0, s, 0, h))

    def yt(i, s):
        ref = w.at[:, yi(-s), half(i, h)]
        send((i, "t", s), ref, ref, other(1 - h))

    def yf(i):
        for c in range(4):
            for s, q in ((1, 0), (-1, 1)):
                got((i, "f", c, s), w.at[zi(SIDES[c]), yi(2), quarter(i, h, q)])
        yt(i, 2)

    def last(i):
        for c in range(1, 4):
            got((i, "s", c), w.at[zi(SIDES[c]), y, half(i, 1 - h)])
        for s in (1, -1, 2):
            got((i, "t", s), w.at[:, yi(-s), half(i, 1 - h)])

    def elementwise():
        down_col[...] = jnp.broadcast_to(ds_ref[...], (LANES, FFL)).T

        @pl.when(home)
        def _():
            for k, ref in enumerate((gs_ref, us_ref, ds_ref)):
                scales[k] = jnp.broadcast_to(ref[...], (LANES, FFL)).T
            send_if(True, ("scales",), lambda: (scales, scales, other(1 - h)))
            loads[3].wait()
            loads[4].wait()

        @pl.when(guest)
        def _():
            got(("scales",), scales)
            swapped(gate, "gate", False)
            swapped(up, "up", False)

        def body(i, n):
            rows = span(i, n)
            g = gate[rows, :].astype(F32)
            u = up[rows, :].astype(F32)
            sig = jax.nn.sigmoid(g)
            act = g * sig
            hidden[rows, :] = (act * u).astype(BF16)
            down = scales[2, rows]
            gs = jnp.concatenate([scales[0, rows] * down] * 4, axis=1)
            us = jnp.concatenate([scales[1, rows] * down] * 4, axis=1)
            fg[rows, :] = u * sig * (1.0 + g * (1.0 - sig)) * gs
            fu[rows, :] = act * us

        chunks(FFL, 16, body)

    def down_grads():
        @pl.loop(0, 8)
        def _(k):
            zz, yy = lax.div(k, 2), lax.rem(k, 2) * 2
            cols = pl.ds(pl.multiple_of(k * 256, 256), 256)
            out = jnp.dot(hidden[...], cot[:, cols], preferred_element_type=F32).astype(BF16)
            grad[zz, yy, pl.ds(0, FFL)] = out[:, :LANES]
            grad[zz, yy + 1, pl.ds(0, FFL)] = out[:, LANES:]

    def cotangents():
        @pl.loop(0, 2)
        def _(m):
            cols = pl.ds(pl.multiple_of(m * 256, 256), 256)
            whole = jnp.concatenate(
                [w[i // 4, i % 4, pl.ds(0, FFL)] for i in range(16)], axis=1
            )
            hc = lax.dot_general(
                whole, cot[cols, :], (((1,), (1,)), ((), ())), preferred_element_type=F32
            )
            bc[pl.ds(0, FFL), cols] = (hc * fg[:, cols]).astype(BF16)
            bc[pl.ds(FFL, FFL), cols] = (hc * fu[:, cols]).astype(BF16)

    def gate_up_grads(i):
        @pl.loop(0, 8)
        def _(k):
            zz, yy = lax.div(k, 2), lax.rem(k, 2) * 2
            cols = pl.ds(pl.multiple_of(k * 256, 256), 256)
            units = pl.ds((i - 1) * FFL, FFL)
            out = jnp.dot(bc[units, :], x[:, cols], preferred_element_type=F32).astype(BF16)
            grad[zz, yy, pl.ds(i * FFL, FFL)] = out[:, :LANES]
            grad[zz, yy + 1, pl.ds(i * FFL, FFL)] = out[:, LANES:]

    def presum(i):
        for k in (2, 1, -1, 0):
            src = grad.at[:, yi(k), half(i, 1 - h)]
            send((i, "ps", k), src, sib.at[:, yi(k), small(i)], other(1 - h))

    def add(i, k, b, *more):
        def body(j, n):
            at = (b, yi(k), span(i * FFL + h * H + j, n))
            total = grad[at].astype(F32) + sib[b, yi(k), span(i * H + j, n)].astype(F32)
            for ref in more:
                total = total + ref[span(i * H + j, n)].astype(F32)
            grad[at] = total.astype(BF16)

        chunks(H, Q, body)

    def part(i, k, b):
        return grad.at[pl.ds(b, 2), yi(k), half(i, h)]

    def got_sib(i, k):
        got((i, "ps", k), sib.at[:, yi(k), small(i)])

    def rs_start(i):
        got_sib(i, 2)
        for b in range(2):
            add(i, 2, b)
        send((i, "r", 0), part(i, 2, 0), r1.at[0, :, small(i)], dev(0, 1, 0, h))
        for b in range(2, 4):
            add(i, 2, b)
        send((i, "r", 1), part(i, 2, 2), r1.at[1, :, small(i)], dev(0, -1, 0, h))
        got_sib(i, 1)
        for b in range(2, 4):
            add(i, 1, b)
        send((i, "r", 2), part(i, 1, 2), r2.at[0, pl.ds(2, 2), small(i)], dev(0, 1, 0, h))
        got_sib(i, -1)
        for b in range(2):
            add(i, -1, b)
        send((i, "r", 3), part(i, -1, 0), r2.at[1, pl.ds(0, 2), small(i)], dev(0, -1, 0, h))

    def rs_plus(i):
        got((i, "r", 0), r1.at[0, :, small(i)])
        for b in range(2):
            add(i, 1, b, r1.at[0, b])
        send((i, "r", 4), part(i, 1, 0), r2.at[0, pl.ds(0, 2), small(i)], dev(0, 1, 0, h))

    def rs_minus(i):
        got((i, "r", 1), r1.at[1, :, small(i)])
        for b in range(2, 4):
            add(i, -1, b, r1.at[1, b - 2])
        send((i, "r", 5), part(i, -1, 2), r2.at[1, pl.ds(2, 2), small(i)], dev(0, -1, 0, h))

    def sum_own(i, k):
        b = zi(k)

        def body(j, n):
            rows = span(i * H + j, n)
            total = grad[b, yi(0), span(i * FFL + h * H + j, n)].astype(F32)
            total = total + sib[b, yi(0), rows].astype(F32)
            total = total + r2[0, b, rows].astype(F32) + r2[1, b, rows].astype(F32)
            own[b, rows] = total.astype(BF16)

        chunks(H, Q, body)

    def rs_own(i):
        got_sib(i, 0)
        got((i, "r", 2), r2.at[0, pl.ds(2, 2), small(i)])
        got((i, "r", 3), r2.at[1, pl.ds(0, 2), small(i)])
        got((i, "r", 4), r2.at[0, pl.ds(0, 2), small(i)])
        got((i, "r", 5), r2.at[1, pl.ds(2, 2), small(i)])
        sum_own(i, 2)
        for q, s in ((0, 2), (1, -2)):
            src = own.at[zi(2), pl.ds(i * H + q * Q, Q)]
            send((i, "g", q), src, zr.at[q, quarter(i, h, q)], dev(0, 0, s, p), by=h)
        for q, s in ((0, 1), (1, -1)):
            sum_own(i, s)
            src = own.at[zi(s), small(i)]
            send((i, "n", q), src, zr.at[q, half(i, h)], dev(0, 0, s, p), by=h)
        sum_own(i, 0)

        @pl.when(guest)
        def _():
            send_if(
                False, (i, "zs"), lambda: (own.at[zl, small(i)], zs.at[small(i)], other(p))
            )

    def rs_fin(i):
        @pl.when(home)
        def _():
            for k in range(2):
                for q in range(2):
                    got((i, "g", q), zr.at[q, quarter(i, k, q)], by=k)
            got((i, "zs"), zs.at[small(i)])
            for q in range(2):
                def body(j, n, q=q):
                    low = span(i * H + q * Q + j, n)
                    rows = span(i * FFL + h * H + q * Q + j, n)
                    total = own[zl, low].astype(F32) + zr[q, rows].astype(F32)
                    final[rows] = total.astype(BF16)
                    rows = span(i * FFL + (1 - h) * H + q * Q + j, n)
                    total = zs[low].astype(F32) + zr[q, rows].astype(F32)
                    final[rows] = total.astype(BF16)

                chunks(Q, Q, body)

        @pl.when(guest)
        def _():
            for k in range(2):
                for q in range(2):
                    got((i, "n", q), zr.at[q, half(i, k)], by=k)

            def body(j, n):
                rows = span(i * FFL + j, n)
                total = zr[0, rows].astype(F32) + zr[1, rows].astype(F32)
                final[rows] = total.astype(BF16)

            chunks(FFL, Q, body)

        for q, s in ((0, 2), (1, -2)):
            send((i, "e", q), final.at[half(i, q)], q1.at[q, small(i)], dev(0, 0, s, h))

    def relay(i, q):
        got((i, "e", q), q1.at[q, small(i)])
        s = (2, -2)[q]
        send((i, "k", q), q1.at[q, small(i)], q2.at[half(i, q)], dev(0, 0, s, h))

    def arrive(i):
        for q in range(2):
            got((i, "k", q), q2.at[half(i, q)])
        out_ref = (od_ref, og_ref, ou_ref)[i]

        def body(j, n):
            rows = span(i * FFL + j, n)
            total = final[rows].astype(F32) + q2[rows].astype(F32)
            if i == 0:
                total = total * down_col[span(j, n)]
            out_ref[span(j, n), :] = total

        chunks(FFL, Q, body)

    def partial_inputs():
        @pl.loop(0, 8)
        def _(r):
            t = lax.rem(xx * 2 + r, 8)
            zz, yy = lax.div(t, 2), lax.rem(t, 2) * 2
            rows = pl.ds(FFL, GU)
            both = jnp.concatenate([w[zz, yy, rows], w[zz, yy + 1, rows]], axis=1)
            value = lax.dot_general(
                bc[...], both, (((0,), (0,)), ((), ())), preferred_element_type=F32
            )
            tp_out[lax.div(r, 2), lax.rem(r, 2)] = value.astype(BF16)

        for k, s in ((0, 1), (1, -1)):
            send(("p", k), tp_out.at[2, :, tokens[k]], xr1.at[k], dev(s, 0, 0, h))
        send(("p", 2), tp_out.at[1, :, tokens[1]], xr2.at[0, :, tokens[1]], dev(1, 0, 0, h))
        send(("p", 3), tp_out.at[3, :, tokens[0]], xr2.at[1, :, tokens[0]], dev(-1, 0, 0, h))

    tokens = (pl.ds(0, HT), pl.ds(HT, HT))

    def partial_on(k):
        s = (1, -1)[k]
        got(("p", k), xr1.at[k])
        for core in range(2):
            def body(j, n, core=core):
                at = (s % 4, core, span(k * HT + j, n))
                total = tp_out[at].astype(F32) + xr1[k, core, span(j, n)].astype(F32)
                tp_out[at] = total.astype(BF16)

            chunks(HT, 128, body)
        send(
            ("p", 4 + k), tp_out.at[s % 4, :, tokens[k]], xr2.at[k, :, tokens[k]],
            dev(s, 0, 0, h),
        )

    def partial_sum():
        got(("p", 2), xr2.at[0, :, tokens[1]])
        got(("p", 3), xr2.at[1, :, tokens[0]])
        got(("p", 4), xr2.at[0, :, tokens[0]])
        got(("p", 5), xr2.at[1, :, tokens[1]])
        for core in range(2):
            def body(j, n, core=core):
                rows = span(j, n)
                total = tp_out[0, core, rows].astype(F32) + xr2[0, core, rows].astype(F32)
                total = total + xr2[1, core, rows].astype(F32)
                tp_out[0, core, rows] = total.astype(BF16)

            chunks(TOK, 128, body)

        @pl.when(home)
        def _():
            send_if(
                True, ("h",), lambda: (tp_out.at[0, 1 - h], from_home, other(1 - h))
            )

            def keep(j, n):
                from_home[span(j, n)] = tp_out[0, h, span(j, n)]

            chunks(TOK, 128, keep)

        @pl.when(guest)
        def _():
            for core in range(2):
                for s, rows in ((-1, tokens[0]), (1, tokens[1])):
                    def make(core=core, s=s, rows=rows):
                        return tp_out.at[0, core, rows], from_guest.at[rows], dev(0, 0, s, core)

                    send_if(False, ("g", s), make, core)

    def input_grad():
        @pl.when(guest)
        def _():
            got(("h",), from_home)

        for s, rows in ((-1, tokens[0]), (1, tokens[1])):
            got(("g", s), from_guest.at[rows])

        def body(j, n):
            rows = span(j, n)
            total = from_home[rows].astype(F32) + from_guest[rows].astype(F32)
            oi_ref[rows, :] = total.astype(BF16)

        chunks(TOK, 128, body)

    work = {
        "st": start, "ys": ys, "yr": yr, "yt": yt, "yf": yf, "last": last,
        "ew": elementwise, "down": down_grads, "hc": cotangents, "gu": gate_up_grads,
        "part": partial_inputs, "p": partial_on, "psum": partial_sum, "tp": input_grad, "ps": presum, "rs": rs_start,
        "r+": rs_plus, "r-": rs_minus, "own": rs_own, "fin": rs_fin, "y": relay, "arr": arrive,
        "sgu": lambda: (swap(gate_hbm, gate, "gate", False), swap(up_hbm, up, "up", False)),
        "sc": lambda: swap(cot_hbm, cot, "cot", True),
        "sx": lambda: swap(x_hbm, x, "x", True),
        "c0": lambda: spread0(cot, "cot"), "c1": lambda: spread1(cot, "cot"),
        "c2": lambda: spread2(cot, "cot", 5),
        "x0": lambda: spread0(x, "x"), "x1": lambda: spread1(x, "x"),
        "x2": lambda: spread2(x, "x", 6),
    }
    for step in ORDER:
        name, *args = step.split(" ")
        work[name](*(int(a) for a in args))
    assert len(send_ids) <= SEMS and sum(recv_sizes) <= SEMS, (len(send_ids), sum(recv_sizes))

    for cond in (None, True, False):
        def drain(cond=cond):
            for c, make, s in sends:
                if c is cond:
                    src, dst, peer = make()
                    remote(src, dst, s, 0, peer).wait_send()

        if cond is None:
            drain()
        else:
            pl.when(home if cond else guest)(drain)


SEMS = 256


def local(
    inputs, cotangent, gate_pre, up_pre, gate_weight, up_weight, down_weight,
    gate_scale, up_scale, down_scale,
):
    hbm = pl.BlockSpec(memory_space=pl.ANY)
    vmem = pl.BlockSpec(memory_space=pltpu.VMEM)
    sem = pltpu.SemaphoreType.DMA
    half = ALL // 2
    oi, og, ou, od = pl.pallas_call(
        kernel,
        out_shape=(
            jax.ShapeDtypeStruct((TOK, 256), BF16),
            jax.ShapeDtypeStruct((FFL, LANES), F32),
            jax.ShapeDtypeStruct((FFL, LANES), F32),
            jax.ShapeDtypeStruct((FFL, LANES), F32),
        ),
        in_specs=[hbm] * 7 + [vmem] * 3,
        out_specs=(vmem,) * 4,
        scratch_shapes=[
            pltpu.VMEM((TOK, D), BF16),
            pltpu.VMEM((TOK, D), BF16),
            pltpu.VMEM((FFL, TOK), BF16),
            pltpu.VMEM((FFL, TOK), BF16),
            pltpu.VMEM((ALL, LANES), F32),
            pltpu.VMEM((3, FFL, LANES), F32),
            pltpu.VMEM((FFL, LANES), F32),
            pltpu.VMEM((FFL, TOK), BF16),
            pltpu.VMEM((FFL, TOK), F32),
            pltpu.VMEM((FFL, TOK), F32),
            pltpu.VMEM((GU, TOK), BF16),
            pltpu.VMEM((4, 4, ALL, LANES), BF16),
            pltpu.VMEM((ALL, LANES), BF16),
            pltpu.VMEM((4, 4, ALL, LANES), BF16),
            pltpu.VMEM((4, 4, half, LANES), BF16),
            pltpu.VMEM((2, 2, half, LANES), BF16),
            pltpu.VMEM((2, 4, half, LANES), BF16),
            pltpu.VMEM((4, half, LANES), BF16),
            pltpu.VMEM((2, ALL, LANES), BF16),
            pltpu.VMEM((half, LANES), BF16),
            pltpu.VMEM((ALL, LANES), BF16),
            pltpu.VMEM((2, half, LANES), BF16),
            pltpu.VMEM((ALL, LANES), BF16),
            pltpu.VMEM((4, 2, TOK, 256), BF16),
            pltpu.VMEM((2, 2, HT, 256), BF16),
            pltpu.VMEM((2, 2, TOK, 256), BF16),
            pltpu.VMEM((TOK, 256), BF16),
            pltpu.VMEM((TOK, 256), BF16),
            sem((7,)),
            sem((SEMS,)),
            sem((SEMS,)),
        ],
        compiler_params=pltpu.CompilerParams(
            collective_id=0, has_side_effects=True, vmem_limit_bytes=58 * 1024 * 1024
        ),
    )(
        inputs, cotangent, gate_pre.T, up_pre.T,
        down_weight.T, gate_weight.T, up_weight.T, gate_scale, up_scale, down_scale,
    )
    return oi, og.T, ou.T, od.T


def solution(mesh):
    rows = ("rep", "fs")
    in_specs = (
        P(rows, None), P(rows, None), P(rows, "tp"), P(rows, "tp"),
        P("fs", "tp"), P("fs", "tp"), P("fs", "tp"),
        P(None, "tp"), P(None, "tp"), P(None, "tp"),
    )
    out_specs = (P(rows, "tp"), P("fs", "tp"), P("fs", "tp"), P("fs", "tp"))
    return jax.shard_map(local, mesh=mesh, in_specs=in_specs, out_specs=out_specs, check_vma=False)
```

```python
import jax
import jax.numpy as jnp
from jax import lax
from jax.experimental import pallas as pl
from jax.experimental.pallas import tpu as pltpu
from jax.sharding import PartitionSpec as P

MESH = pl.DeviceIdType.MESH
F32 = jnp.float32
BF16 = jnp.bfloat16
LANES = 128
TOK = 512
HT = TOK // 2
D = 2048
QD = D // 4
FFL = 704
GU = 2 * FFL
ALL = 3 * FFL
SIDES = (0, -1, 1, 2)

PIECES = ((0, 704), (704, 704), (1408, 704))
ORDER = (
    "st 1", "sc", "st 0", "ys 1 0", "st 2", "ys 2 0", "yr 1 0 1", "ys 0 0", "yr 1 0 -1",
    "ys 1 1", "ys 1 2", "sgu", "ys 1 3", "c0", "ys 0 3", "ys 0 2", "ys 2 3", "yr 0 3 -1",
    "ys 0 1", "c1", "yr 1 2 1", "yr 0 2 1", "sx", "yr 0 3 1", "yr 1 2 -1", "ys 2 2",
    "yr 1 3 1", "yr 2 0 -1", "ew", "yr 0 1 1", "yr 0 0 -1", "c2", "yr 0 2 -1", "yr 1 3 -1",
    "yr 1 1 -1", "yr 2 0 1", "yr 0 0 1", "ys 2 1", "yt 0 1", "down", "ps 0", "x0", "yr 0 1 -1",
    "yr 2 3 1", "rs 0", "yf 0", "yt 0 -1", "yr 2 2 1", "last 0", "yr 2 2 -1", "x1", "hc",
    "r+ 0", "yr 2 1 1", "r- 0", "yr 1 1 1", "yt 1 -1", "yt 2 1", "x2", "yr 2 3 -1",
    "yr 2 1 -1", "yt 1 1", "gu 1", "ps 1", "rs 1", "own 0", "gu 2", "ps 2", "r- 1", "r+ 1",
    "yf 2", "yf 1", "yt 2 -1", "fin 0", "rs 2", "last 2", "own 1", "y 0 1", "y 0 0", "last 1",
    "part", "r- 2", "r+ 2", "fin 1", "own 2", "y 1 1", "p 1", "y 1 0", "p 0", "fin 2", "psum",
    "arr 1", "y 2 0", "y 2 1", "arr 0", "tp", "arr 2",
)

def kernel(
    x_hbm, cot_hbm, gate_hbm, up_hbm, wd_hbm, wg_hbm, wu_hbm, gs_ref, us_ref, ds_ref,
    oi_ref, out_ref,
    x, cot, gate, up, w32, scales, down_col, hidden, fg, fu, bc,
    w, mine, grad, sib, r1, r2, own, zr, zs, final, q1, q2,
    tp_out, xr1, xr2, from_home, from_guest,
    local_sem, send_sem, recv_sem,
):
    rep = lax.axis_index("rep")
    fs = lax.axis_index("fs")
    tp = lax.axis_index("tp")
    y = lax.rem(fs, 4)
    zl = lax.div(fs, 4)
    z = rep * 4 + zl
    xx = lax.div(tp, 2)
    h = lax.rem(tp, 2)
    p = lax.rem(zl, 2)
    home = h == p
    guest = h != p

    def dev(dx, dy, dz, core):
        nx = lax.rem(xx + dx + 4, 4)
        ny = lax.rem(y + dy + 4, 4)
        nz = lax.rem(z + dz + 8, 8)
        return (lax.div(nz, 4), lax.rem(nz, 4) * 4 + ny, nx * 2 + core)

    def yi(k):
        return lax.rem(y + k + 4, 4)

    def zi(k):
        return lax.rem(zl + k + 4, 4)

    def chunks(n, size, fn):
        if n == size:
            fn(0, size)
            return

        @pl.loop(0, n // size)
        def _(i):
            fn(i * size, size)

    def span(start, size):
        return pl.ds(start if isinstance(start, int) else pl.multiple_of(start, 16), size)

    def whole(i):
        lo, n = PIECES[i]
        return pl.ds(lo, n)

    def half(i, k):
        lo, n = PIECES[i]
        return pl.ds(pl.multiple_of(lo + k * (n // 2), 16), n // 2)

    def quarter(i, k, q):
        lo, n = PIECES[i]
        return pl.ds(pl.multiple_of(lo + k * (n // 2) + q * (n // 4), 16), n // 4)

    def small(i):
        lo, n = PIECES[i]
        return pl.ds(lo // 2, n // 2)

    send_ids, recv_ids = {}, {}
    sends = []

    def remote(src, dst, s, r, peer):
        return pltpu.make_async_remote_copy(
            src_ref=src, dst_ref=dst, send_sem=send_sem.at[s], recv_sem=recv_sem.at[r],
            device_id=peer, device_id_type=MESH,
        )

    def rid(name, spread):
        key = name if spread is None else (*name, "by")
        if key not in recv_ids:
            recv_ids[key] = sum(recv_sizes)
            recv_sizes.append(1 if spread is None else 2)
        return recv_ids[key] if spread is None else recv_ids[key] + spread

    recv_sizes = []

    def send(name, src, dst, peer, tag="", by=None):
        s = send_ids.setdefault((*name, tag), len(send_ids))
        remote(src, dst, s, rid(name, by), peer).start()
        sends.append((None, lambda: (src, dst, peer), s))

    def send_if(cond, name, make, tag=""):
        s = send_ids.setdefault((*name, tag), len(send_ids))
        src, dst, peer = make()
        remote(src, dst, s, rid(name, None), peer).start()
        sends.append((cond, make, s))

    def got(name, dst, by=None):
        remote(dst, dst, 0, rid(name, by), dev(0, 1, 0, h)).wait_recv()

    loads = []
    for k, (src, dst) in enumerate(
        (
            (wd_hbm, w32.at[pl.ds(0, FFL)]),
            (wg_hbm, w32.at[pl.ds(FFL, FFL)]),
            (wu_hbm, w32.at[pl.ds(GU, FFL)]),
            (gate_hbm, gate),
            (up_hbm, up),
            (cot_hbm, cot),
            (x_hbm, x),
        )
    ):
        loads.append(pltpu.make_async_copy(src, dst, local_sem.at[k]))
    for k in range(3):
        loads[k].start()

    barrier = pltpu.get_barrier_semaphore()
    peers = [dev(0, 1, 0, h), dev(0, -1, 0, h), dev(1, 0, 0, h), dev(-1, 0, 0, h)]
    for core in range(2):
        peers += [dev(0, 0, k, core) for k in (1, -1, 2, -2)]
    peers.append(dev(0, 0, 0, 1 - h))
    for peer in peers:
        pl.semaphore_signal(barrier, inc=1, device_id=peer, device_id_type=MESH)

    @pl.when(home)
    def _():
        for k in range(3, 7):
            loads[k].start()

    for k in range(3):
        loads[k].wait()

    @pl.when(home)
    def _():
        def narrow(i, n):
            w[zl, y, span(i, n)] = w32[span(i, n)].astype(BF16)

        chunks(ALL, 176, narrow)

    @pl.when(guest)
    def _():
        def narrow(i, n):
            mine[span(i, n)] = w32[span(i, n)].astype(BF16)

        chunks(ALL, 176, narrow)

    pl.semaphore_wait(barrier, len(peers))

    def other(core):
        return dev(0, 0, 0, core)

    def start(i):
        @pl.when(home)
        def _():
            send_if(
                True, (i, "own"),
                lambda: (w.at[zl, y, whole(i)], w.at[zl, y, whole(i)], other(1 - h)),
            )
            for k in range(2):
                for q, s in ((0, 2), (1, -2)):
                    def make(k=k, q=q, s=s):
                        ref = w.at[zl, y, quarter(i, k, q)]
                        return ref, ref, dev(0, 0, s, k)

                    send_if(True, (i, "zq", q), make, k)

        @pl.when(guest)
        def _():
            for k in range(2):
                for s in (1, -1):
                    def make(k=k, s=s):
                        rows = half(i, k)
                        return mine.at[rows], w.at[zl, y, rows], dev(0, 0, s, k)

                    send_if(False, (i, "z", s), make, k)

    def swap(src, dst, name, wide):
        @pl.when(guest)
        def _():
            for s, part in ((1, pl.ds(0, HT)), (-1, pl.ds(HT, HT))):
                def make(s=s, part=part):
                    at = (part, qcols(0)) if wide else (slice(None), part)
                    return src.at[at], dst.at[at], dev(0, 0, s, p)

                send_if(False, (name, s), make)

    def swapped(dst, name, wide):
        for s, part in ((1, pl.ds(0, HT)), (-1, pl.ds(HT, HT))):
            at = (part, qcols(0)) if wide else (slice(None), part)
            got((name, s), dst.at[at])

    def qcols(k):
        return pl.ds(pl.multiple_of(lax.rem(xx + k + 4, 4) * QD, QD), QD)

    def spread0(dst, name):
        @pl.when(guest)
        def _():
            swapped(dst, name, True)
            for s in (1, -1):
                def make(s=s):
                    ref = dst.at[:, qcols(0)]
                    return ref, ref, dev(s, 0, 0, h)

                send_if(False, (name, "x", s), make)

    def spread1(dst, name):
        @pl.when(guest)
        def _():
            for s, part in ((1, pl.ds(0, HT)), (-1, pl.ds(HT, HT))):
                got((name, "x", s), dst.at[:, qcols(-s)])

                def make(s=s, part=part):
                    ref = dst.at[part, qcols(-s)]
                    return ref, ref, dev(s, 0, 0, h)

                send_if(False, (name, "xf", s), make)

    def spread2(dst, name, load):
        @pl.when(guest)
        def _():
            for s, part in ((1, pl.ds(0, HT)), (-1, pl.ds(HT, HT))):
                got((name, "xf", s), dst.at[part, qcols(2)])

        @pl.when(home)
        def _():
            loads[load].wait()

    def ys(i, c):
        ref = w.at[zi(SIDES[c]), y, half(i, h)]
        if c == 0:
            @pl.when(guest)
            def _():
                got((i, "own"), w.at[zl, y, whole(i)])
        elif c < 3:
            got((i, "z", -SIDES[c]), ref)
        else:
            for q in range(2):
                got((i, "zq", q), w.at[zi(2), y, quarter(i, h, q)])
        for s in (1, -1):
            send((i, "y", c, s), ref, ref, dev(0, s, 0, h))
        if c:
            send((i, "s", c), ref, ref, other(1 - h))

    def yr(i, c, s):
        got((i, "y", c, s), w.at[zi(SIDES[c]), yi(-s), half(i, h)])
        q = 0 if s == 1 else 1
        ref = w.at[zi(SIDES[c]), yi(-s), quarter(i, h, q)]
        send((i, "f", c, s), ref, ref, dev(0, s, 0, h))

    def yt(i, s):
        ref = w.at[:, yi(-s), half(i, h)]
        send((i, "t", s), ref, ref, other(1 - h))

    def yf(i):
        for c in range(4):
            for s, q in ((1, 0), (-1, 1)):
                got((i, "f", c, s), w.at[zi(SIDES[c]), yi(2), quarter(i, h, q)])
        yt(i, 2)

    def last(i):
        for c in range(1, 4):
            got((i, "s", c), w.at[zi(SIDES[c]), y, half(i, 1 - h)])
        for s in (1, -1, 2):
            got((i, "t", s), w.at[:, yi(-s), half(i, 1 - h)])

    def elementwise():
        down_col[...] = jnp.broadcast_to(ds_ref[...], (LANES, FFL)).T

        @pl.when(home)
        def _():
            for k, ref in enumerate((gs_ref, us_ref, ds_ref)):
                scales[k] = jnp.broadcast_to(ref[...], (LANES, FFL)).T
            send_if(True, ("scales",), lambda: (scales, scales, other(1 - h)))
            loads[3].wait()
            loads[4].wait()

        @pl.when(guest)
        def _():
            got(("scales",), scales)
            swapped(gate, "gate", False)
            swapped(up, "up", False)

        def body(i, n):
            rows = span(i, n)
            g = gate[rows, :].astype(F32)
            u = up[rows, :].astype(F32)
            sig = jax.nn.sigmoid(g)
            act = g * sig
            hidden[rows, :] = (act * u).astype(BF16)
            down = scales[2, rows]
            gs = jnp.concatenate([scales[0, rows] * down] * 4, axis=1)
            us = jnp.concatenate([scales[1, rows] * down] * 4, axis=1)
            fg[rows, :] = u * sig * (1.0 + g * (1.0 - sig)) * gs
            fu[rows, :] = act * us

        chunks(FFL, 16, body)

    def down_grads():
        @pl.loop(0, 8)
        def _(k):
            zz, yy = lax.div(k, 2), lax.rem(k, 2) * 2
            cols = pl.ds(pl.multiple_of(k * 256, 256), 256)
            out = jnp.dot(hidden[...], cot[:, cols], preferred_element_type=F32).astype(BF16)
            grad[zz, yy, pl.ds(0, FFL)] = out[:, :LANES]
            grad[zz, yy + 1, pl.ds(0, FFL)] = out[:, LANES:]

    def cotangents():
        @pl.loop(0, 2)
        def _(m):
            cols = pl.ds(pl.multiple_of(m * 256, 256), 256)
            rows = jnp.concatenate(
                [w[i // 4, i % 4, pl.ds(0, FFL)] for i in range(16)], axis=1
            )
            hc = lax.dot_general(
                rows, cot[cols, :], (((1,), (1,)), ((), ())), preferred_element_type=F32
            )
            bc[pl.ds(0, FFL), cols] = (hc * fg[:, cols]).astype(BF16)
            bc[pl.ds(FFL, FFL), cols] = (hc * fu[:, cols]).astype(BF16)

    def gate_up_grads(i):
        @pl.loop(0, 8)
        def _(k):
            zz, yy = lax.div(k, 2), lax.rem(k, 2) * 2
            cols = pl.ds(pl.multiple_of(k * 256, 256), 256)
            lo, n = PIECES[i]
            out = jnp.dot(bc[pl.ds(lo - FFL, n), :], x[:, cols], preferred_element_type=F32).astype(BF16)
            grad[zz, yy, whole(i)] = out[:, :LANES]
            grad[zz, yy + 1, whole(i)] = out[:, LANES:]

    def presum(i):
        for k in (2, 1, -1, 0):
            src = grad.at[:, yi(k), half(i, 1 - h)]
            send((i, "ps", k), src, sib.at[:, yi(k), small(i)], other(1 - h))

    def add(i, k, b, *more):
        lo, size = PIECES[i]

        def body(j, n):
            at = (b, yi(k), span(lo + h * (size // 2) + j, n))
            low = span(lo // 2 + j, n)
            total = grad[at].astype(F32) + sib[b, yi(k), low].astype(F32)
            for ref in more:
                total = total + ref[low].astype(F32)
            grad[at] = total.astype(BF16)

        chunks(size // 2, size // 4, body)

    def part(i, k, b):
        return grad.at[pl.ds(b, 2), yi(k), half(i, h)]

    def got_sib(i, k):
        got((i, "ps", k), sib.at[:, yi(k), small(i)])

    def rs_start(i):
        got_sib(i, 2)
        for b in range(2):
            add(i, 2, b)
        send((i, "r", 0), part(i, 2, 0), r1.at[0, :, small(i)], dev(0, 1, 0, h))
        for b in range(2, 4):
            add(i, 2, b)
        send((i, "r", 1), part(i, 2, 2), r1.at[1, :, small(i)], dev(0, -1, 0, h))
        got_sib(i, 1)
        for b in range(2, 4):
            add(i, 1, b)
        send((i, "r", 2), part(i, 1, 2), r2.at[0, pl.ds(2, 2), small(i)], dev(0, 1, 0, h))
        got_sib(i, -1)
        for b in range(2):
            add(i, -1, b)
        send((i, "r", 3), part(i, -1, 0), r2.at[1, pl.ds(0, 2), small(i)], dev(0, -1, 0, h))

    def rs_plus(i):
        got((i, "r", 0), r1.at[0, :, small(i)])
        for b in range(2):
            add(i, 1, b, r1.at[0, b])
        send((i, "r", 4), part(i, 1, 0), r2.at[0, pl.ds(0, 2), small(i)], dev(0, 1, 0, h))

    def rs_minus(i):
        got((i, "r", 1), r1.at[1, :, small(i)])
        for b in range(2, 4):
            add(i, -1, b, r1.at[1, b - 2])
        send((i, "r", 5), part(i, -1, 2), r2.at[1, pl.ds(2, 2), small(i)], dev(0, -1, 0, h))

    def sum_own(i, k):
        b = zi(k)
        lo, size = PIECES[i]

        def body(j, n):
            rows = span(lo // 2 + j, n)
            total = grad[b, yi(0), span(lo + h * (size // 2) + j, n)].astype(F32)
            total = total + sib[b, yi(0), rows].astype(F32)
            total = total + r2[0, b, rows].astype(F32) + r2[1, b, rows].astype(F32)
            own[b, rows] = total.astype(BF16)

        chunks(size // 2, size // 4, body)

    def rs_own(i):
        got_sib(i, 0)
        got((i, "r", 2), r2.at[0, pl.ds(2, 2), small(i)])
        got((i, "r", 3), r2.at[1, pl.ds(0, 2), small(i)])
        got((i, "r", 4), r2.at[0, pl.ds(0, 2), small(i)])
        got((i, "r", 5), r2.at[1, pl.ds(2, 2), small(i)])
        lo, n = PIECES[i]
        sum_own(i, 2)
        for q, s in ((0, 2), (1, -2)):
            src = own.at[zi(2), pl.ds(lo // 2 + q * (n // 4), n // 4)]
            send((i, "g", q), src, zr.at[q, quarter(i, h, q)], dev(0, 0, s, p), by=h)
        for q, s in ((0, 1), (1, -1)):
            sum_own(i, s)
            src = own.at[zi(s), small(i)]
            send((i, "n", q), src, zr.at[q, half(i, h)], dev(0, 0, s, p), by=h)
        sum_own(i, 0)

        @pl.when(guest)
        def _():
            send_if(
                False, (i, "zs"), lambda: (own.at[zl, small(i)], zs.at[small(i)], other(p))
            )

    def rs_fin(i):
        lo, size = PIECES[i]
        hn, qn = size // 2, size // 4

        @pl.when(home)
        def _():
            for k in range(2):
                for q in range(2):
                    got((i, "g", q), zr.at[q, quarter(i, k, q)], by=k)
            got((i, "zs"), zs.at[small(i)])
            for q in range(2):
                def body(j, n, q=q):
                    low = span(lo // 2 + q * qn + j, n)
                    rows = span(lo + h * hn + q * qn + j, n)
                    total = own[zl, low].astype(F32) + zr[q, rows].astype(F32)
                    final[rows] = total.astype(BF16)
                    rows = span(lo + (1 - h) * hn + q * qn + j, n)
                    total = zs[low].astype(F32) + zr[q, rows].astype(F32)
                    final[rows] = total.astype(BF16)

                chunks(qn, qn, body)

        @pl.when(guest)
        def _():
            for k in range(2):
                for q in range(2):
                    got((i, "n", q), zr.at[q, half(i, k)], by=k)

            def body(j, n):
                rows = span(lo + j, n)
                total = zr[0, rows].astype(F32) + zr[1, rows].astype(F32)
                final[rows] = total.astype(BF16)

            chunks(size, qn, body)

        for q, s in ((0, 2), (1, -2)):
            send((i, "e", q), final.at[half(i, q)], q1.at[q, small(i)], dev(0, 0, s, h))

    def relay(i, q):
        got((i, "e", q), q1.at[q, small(i)])
        s = (2, -2)[q]
        send((i, "k", q), q1.at[q, small(i)], q2.at[half(i, q)], dev(0, 0, s, h))

    def arrive(i):
        for q in range(2):
            got((i, "k", q), q2.at[half(i, q)])
        lo, size = PIECES[i]

        def body(j, n):
            rows = span(lo + j, n)
            total = final[rows].astype(F32) + q2[rows].astype(F32)
            if lo < FFL:
                total = total * down_col[rows]
            out_ref[rows, :] = total

        chunks(size, size // 4, body)

    def partial_inputs():
        @pl.loop(0, 8)
        def _(r):
            t = lax.rem(xx * 2 + r, 8)
            zz, yy = lax.div(t, 2), lax.rem(t, 2) * 2
            rows = pl.ds(FFL, GU)
            both = jnp.concatenate([w[zz, yy, rows], w[zz, yy + 1, rows]], axis=1)
            value = lax.dot_general(
                bc[...], both, (((0,), (0,)), ((), ())), preferred_element_type=F32
            )
            tp_out[lax.div(r, 2), lax.rem(r, 2)] = value.astype(BF16)

        for k, s in ((0, 1), (1, -1)):
            send(("p", k), tp_out.at[2, :, tokens[k]], xr1.at[k], dev(s, 0, 0, h))
        send(("p", 2), tp_out.at[1, :, tokens[1]], xr2.at[0, :, tokens[1]], dev(1, 0, 0, h))
        send(("p", 3), tp_out.at[3, :, tokens[0]], xr2.at[1, :, tokens[0]], dev(-1, 0, 0, h))

    tokens = (pl.ds(0, HT), pl.ds(HT, HT))

    def partial_on(k):
        s = (1, -1)[k]
        got(("p", k), xr1.at[k])
        for core in range(2):
            def body(j, n, core=core):
                at = (s % 4, core, span(k * HT + j, n))
                total = tp_out[at].astype(F32) + xr1[k, core, span(j, n)].astype(F32)
                tp_out[at] = total.astype(BF16)

            chunks(HT, 128, body)
        send(
            ("p", 4 + k), tp_out.at[s % 4, :, tokens[k]], xr2.at[k, :, tokens[k]],
            dev(s, 0, 0, h),
        )

    def partial_sum():
        got(("p", 2), xr2.at[0, :, tokens[1]])
        got(("p", 3), xr2.at[1, :, tokens[0]])
        got(("p", 4), xr2.at[0, :, tokens[0]])
        got(("p", 5), xr2.at[1, :, tokens[1]])
        for core in range(2):
            def body(j, n, core=core):
                rows = span(j, n)
                total = tp_out[0, core, rows].astype(F32) + xr2[0, core, rows].astype(F32)
                total = total + xr2[1, core, rows].astype(F32)
                tp_out[0, core, rows] = total.astype(BF16)

            chunks(TOK, 128, body)

        @pl.when(home)
        def _():
            send_if(
                True, ("h",), lambda: (tp_out.at[0, 1 - h], from_home, other(1 - h))
            )

            def keep(j, n):
                from_home[span(j, n)] = tp_out[0, h, span(j, n)]

            chunks(TOK, 128, keep)

        @pl.when(guest)
        def _():
            for core in range(2):
                for s, rows in ((-1, tokens[0]), (1, tokens[1])):
                    def make(core=core, s=s, rows=rows):
                        return tp_out.at[0, core, rows], from_guest.at[rows], dev(0, 0, s, core)

                    send_if(False, ("g", s), make, core)

    def input_grad():
        @pl.when(guest)
        def _():
            got(("h",), from_home)

        for s, rows in ((-1, tokens[0]), (1, tokens[1])):
            got(("g", s), from_guest.at[rows])

        def body(j, n):
            rows = span(j, n)
            total = from_home[rows].astype(F32) + from_guest[rows].astype(F32)
            oi_ref[rows, :] = total.astype(BF16)

        chunks(TOK, 128, body)

    work = {
        "st": start, "ys": ys, "yr": yr, "yt": yt, "yf": yf, "last": last,
        "ew": elementwise, "down": down_grads, "hc": cotangents, "gu": gate_up_grads,
        "part": partial_inputs, "p": partial_on, "psum": partial_sum, "tp": input_grad, "ps": presum, "rs": rs_start,
        "r+": rs_plus, "r-": rs_minus, "own": rs_own, "fin": rs_fin, "y": relay, "arr": arrive,
        "sgu": lambda: (swap(gate_hbm, gate, "gate", False), swap(up_hbm, up, "up", False)),
        "sc": lambda: swap(cot_hbm, cot, "cot", True),
        "sx": lambda: swap(x_hbm, x, "x", True),
        "c0": lambda: spread0(cot, "cot"), "c1": lambda: spread1(cot, "cot"),
        "c2": lambda: spread2(cot, "cot", 5),
        "x0": lambda: spread0(x, "x"), "x1": lambda: spread1(x, "x"),
        "x2": lambda: spread2(x, "x", 6),
    }
    for step in ORDER:
        name, *args = step.split(" ")
        work[name](*(int(a) for a in args))
    assert len(send_ids) <= SEMS and sum(recv_sizes) <= SEMS, (len(send_ids), sum(recv_sizes))

    for cond in (None, True, False):
        def drain(cond=cond):
            for c, make, s in sends:
                if c is cond:
                    src, dst, peer = make()
                    remote(src, dst, s, 0, peer).wait_send()

        if cond is None:
            drain()
        else:
            pl.when(home if cond else guest)(drain)


SEMS = 256


def hand_out(oi_in, all_in, oi_out, og_out, ou_out, od_out, oi, grads, in_sem, out_sem):
    pieces = [(oi_in, oi, oi_out)]
    for k, ref in enumerate((od_out, og_out, ou_out)):
        rows = pl.ds(k * FFL, FFL)
        pieces.append((all_in.at[rows], grads.at[rows], ref))
    copies = []
    for k, (src, mid, dst) in enumerate(pieces):
        first = pltpu.make_async_copy(src, mid, in_sem.at[k])
        first.start()
        copies.append((first, pltpu.make_async_copy(mid, dst, out_sem.at[k])))
    for first, second in copies:
        first.wait()
        second.start()
    for _, second in copies:
        second.wait()


def local(
    inputs, cotangent, gate_pre, up_pre, gate_weight, up_weight, down_weight,
    gate_scale, up_scale, down_scale,
):
    hbm = pl.BlockSpec(memory_space=pl.ANY)
    vmem = pl.BlockSpec(memory_space=pltpu.VMEM)
    sem = pltpu.SemaphoreType.DMA
    half = ALL // 2
    oi, out = pl.pallas_call(
        kernel,
        out_shape=(
            jax.ShapeDtypeStruct((TOK, 256), BF16),
            jax.ShapeDtypeStruct((ALL, LANES), F32),
        ),
        in_specs=[hbm] * 7 + [vmem] * 3,
        out_specs=(vmem,) * 2,
        scratch_shapes=[
            pltpu.VMEM((TOK, D), BF16),
            pltpu.VMEM((TOK, D), BF16),
            pltpu.VMEM((FFL, TOK), BF16),
            pltpu.VMEM((FFL, TOK), BF16),
            pltpu.VMEM((ALL, LANES), F32),
            pltpu.VMEM((3, FFL, LANES), F32),
            pltpu.VMEM((FFL, LANES), F32),
            pltpu.VMEM((FFL, TOK), BF16),
            pltpu.VMEM((FFL, TOK), F32),
            pltpu.VMEM((FFL, TOK), F32),
            pltpu.VMEM((GU, TOK), BF16),
            pltpu.VMEM((4, 4, ALL, LANES), BF16),
            pltpu.VMEM((ALL, LANES), BF16),
            pltpu.VMEM((4, 4, ALL, LANES), BF16),
            pltpu.VMEM((4, 4, half, LANES), BF16),
            pltpu.VMEM((2, 2, half, LANES), BF16),
            pltpu.VMEM((2, 4, half, LANES), BF16),
            pltpu.VMEM((4, half, LANES), BF16),
            pltpu.VMEM((2, ALL, LANES), BF16),
            pltpu.VMEM((half, LANES), BF16),
            pltpu.VMEM((ALL, LANES), BF16),
            pltpu.VMEM((2, half, LANES), BF16),
            pltpu.VMEM((ALL, LANES), BF16),
            pltpu.VMEM((4, 2, TOK, 256), BF16),
            pltpu.VMEM((2, 2, HT, 256), BF16),
            pltpu.VMEM((2, 2, TOK, 256), BF16),
            pltpu.VMEM((TOK, 256), BF16),
            pltpu.VMEM((TOK, 256), BF16),
            sem((7,)),
            sem((SEMS,)),
            sem((SEMS,)),
        ],
        compiler_params=pltpu.CompilerParams(
            collective_id=0, has_side_effects=True, vmem_limit_bytes=58 * 1024 * 1024
        ),
    )(
        inputs, cotangent, gate_pre.T, up_pre.T,
        down_weight.T, gate_weight.T, up_weight.T, gate_scale, up_scale, down_scale,
    )
    oi, og, ou, od = pl.pallas_call(
        hand_out,
        out_shape=(
            jax.ShapeDtypeStruct((TOK, 256), BF16),
            jax.ShapeDtypeStruct((FFL, LANES), F32),
            jax.ShapeDtypeStruct((FFL, LANES), F32),
            jax.ShapeDtypeStruct((FFL, LANES), F32),
        ),
        in_specs=[hbm] * 2,
        out_specs=(hbm,) * 4,
        scratch_shapes=[
            pltpu.VMEM((TOK, 256), BF16), pltpu.VMEM((ALL, LANES), F32), sem((4,)), sem((4,)),
        ],
        compiler_params=pltpu.CompilerParams(vmem_limit_bytes=60 * 1024 * 1024),
    )(oi, out)
    return oi, og.T, ou.T, od.T


def solution(mesh):
    rows = ("rep", "fs")
    in_specs = (
        P(rows, None), P(rows, None), P(rows, "tp"), P(rows, "tp"),
        P("fs", "tp"), P("fs", "tp"), P("fs", "tp"),
        P(None, "tp"), P(None, "tp"), P(None, "tp"),
    )
    out_specs = (P(rows, "tp"), P("fs", "tp"), P("fs", "tp"), P("fs", "tp"))
    return jax.shard_map(local, mesh=mesh, in_specs=in_specs, out_specs=out_specs, check_vma=False)
```

```python
import jax
import jax.numpy as jnp
from jax import lax
from jax.experimental import pallas as pl
from jax.experimental.pallas import tpu as pltpu
from jax.sharding import PartitionSpec as P

MESH = pl.DeviceIdType.MESH
F32 = jnp.float32
BF16 = jnp.bfloat16
LANES = 128
TOK = 512
HT = TOK // 2
D = 2048
QD = D // 4
FFL = 704
GU = 2 * FFL
ALL = 3 * FFL
SIDES = (0, -1, 1, 2)

PIECES = ((0, 704), (704, 704), (1408, 704))
ORDER = (
    "st 2", "sc", "st 0", "ys 0 0", "ys 2 0", "st 1", "ys 1 0", "ys 2 2", "ys 2 1", "ys 0 3",
    "c0", "ys 2 3", "sgu", "sx", "yr 0 0 -1", "ys 1 3", "ys 0 1", "ys 0 2", "ys 1 1", "ys 1 2",
    "c1", "yr 0 1 -1", "yr 0 3 1", "yr 0 2 1", "ew", "yr 2 2 1", "x0", "yr 0 3 -1",
    "yr 2 3 -1", "yr 2 2 -1", "yr 0 2 -1", "yr 2 0 -1", "yr 1 0 -1", "yr 2 1 1", "c2",
    "yr 0 0 1", "yr 0 1 1", "yt 0 -1", "yr 1 2 1", "yr 1 3 -1", "yr 1 1 -1", "yr 1 3 1",
    "yr 1 1 1", "yr 1 2 -1", "yr 1 0 1", "yt 0 1", "down", "yr 2 0 1", "yr 2 1 -1", "ps 0",
    "yf 0", "yt 1 1", "rs 0", "yt 2 -1", "x1", "yr 2 3 1", "last 0", "yf 1", "hc", "x2",
    "r+ 0", "yt 2 1", "r- 0", "gu 1", "yf 2", "ps 1", "rs 1", "own 0", "gu 2", "yt 1 -1",
    "last 2", "r- 1", "ps 2", "r+ 1", "fin 0", "rs 2", "own 1", "last 1", "part", "y 0 1",
    "y 0 0", "fin 1", "r- 2", "r+ 2", "own 2", "y 1 1", "p 1", "y 1 0", "p 0", "fin 2", "psum",
    "y 2 1", "y 2 0", "tp", "arr 1", "arr 0", "arr 2",
)

def kernel(
    x_hbm, cot_hbm, gate_hbm, up_hbm, wd_hbm, wg_hbm, wu_hbm, gs_ref, us_ref, ds_ref,
    oi_ref, out_ref,
    x, cot, gate, up, w32, scales, down_col, hidden, fg, fu, bc,
    w, mine, grad, sib, r1, r2, own, zr, zs, final, q1, q2,
    tp_out, xr1, xr2, from_home, from_guest,
    local_sem, send_sem, recv_sem,
):
    rep = lax.axis_index("rep")
    fs = lax.axis_index("fs")
    tp = lax.axis_index("tp")
    y = lax.rem(fs, 4)
    zl = lax.div(fs, 4)
    z = rep * 4 + zl
    xx = lax.div(tp, 2)
    h = lax.rem(tp, 2)
    p = lax.rem(zl, 2)
    home = h == p
    guest = h != p

    def dev(dx, dy, dz, core):
        nx = lax.rem(xx + dx + 4, 4)
        ny = lax.rem(y + dy + 4, 4)
        nz = lax.rem(z + dz + 8, 8)
        return (lax.div(nz, 4), lax.rem(nz, 4) * 4 + ny, nx * 2 + core)

    def yi(k):
        return lax.rem(y + k + 4, 4)

    def zi(k):
        return lax.rem(zl + k + 4, 4)

    def chunks(n, size, fn):
        if n == size:
            fn(0, size)
            return

        @pl.loop(0, n // size)
        def _(i):
            fn(i * size, size)

    def span(start, size):
        return pl.ds(start if isinstance(start, int) else pl.multiple_of(start, 16), size)

    def whole(i):
        lo, n = PIECES[i]
        return pl.ds(lo, n)

    def half(i, k):
        lo, n = PIECES[i]
        return pl.ds(pl.multiple_of(lo + k * (n // 2), 16), n // 2)

    def quarter(i, k, q):
        lo, n = PIECES[i]
        return pl.ds(pl.multiple_of(lo + k * (n // 2) + q * (n // 4), 16), n // 4)

    def small(i):
        lo, n = PIECES[i]
        return pl.ds(lo // 2, n // 2)

    send_ids, recv_ids = {}, {}
    sends = []

    def remote(src, dst, s, r, peer):
        return pltpu.make_async_remote_copy(
            src_ref=src, dst_ref=dst, send_sem=send_sem.at[s], recv_sem=recv_sem.at[r],
            device_id=peer, device_id_type=MESH,
        )

    def rid(name, spread):
        key = name if spread is None else (*name, "by")
        if key not in recv_ids:
            recv_ids[key] = sum(recv_sizes)
            recv_sizes.append(1 if spread is None else 2)
        return recv_ids[key] if spread is None else recv_ids[key] + spread

    recv_sizes = []

    def send(name, src, dst, peer, tag="", by=None):
        s = send_ids.setdefault((*name, tag), len(send_ids))
        remote(src, dst, s, rid(name, by), peer).start()
        sends.append((None, lambda: (src, dst, peer), s))

    def send_if(cond, name, make, tag=""):
        s = send_ids.setdefault((*name, tag), len(send_ids))
        src, dst, peer = make()
        remote(src, dst, s, rid(name, None), peer).start()
        sends.append((cond, make, s))

    def got(name, dst, by=None):
        remote(dst, dst, 0, rid(name, by), dev(0, 1, 0, h)).wait_recv()

    loads = []
    for k, (src, dst) in enumerate(
        (
            (wd_hbm, w32.at[pl.ds(0, FFL)]),
            (wg_hbm, w32.at[pl.ds(FFL, FFL)]),
            (wu_hbm, w32.at[pl.ds(GU, FFL)]),
            (gate_hbm, gate),
            (up_hbm, up),
            (cot_hbm, cot),
            (x_hbm, x),
        )
    ):
        loads.append(pltpu.make_async_copy(src, dst, local_sem.at[k]))
    for k in range(3):
        loads[k].start()

    barrier = pltpu.get_barrier_semaphore()
    peers = [dev(0, 1, 0, h), dev(0, -1, 0, h), dev(1, 0, 0, h), dev(-1, 0, 0, h)]
    for core in range(2):
        peers += [dev(0, 0, k, core) for k in (1, -1, 2, -2)]
    peers.append(dev(0, 0, 0, 1 - h))
    for peer in peers:
        pl.semaphore_signal(barrier, inc=1, device_id=peer, device_id_type=MESH)

    @pl.when(home)
    def _():
        for k in range(3, 7):
            loads[k].start()

    for k in range(3):
        loads[k].wait()

    @pl.when(home)
    def _():
        def narrow(i, n):
            w[zl, y, span(i, n)] = w32[span(i, n)].astype(BF16)

        chunks(ALL, 176, narrow)

    @pl.when(guest)
    def _():
        def narrow(i, n):
            mine[span(i, n)] = w32[span(i, n)].astype(BF16)

        chunks(ALL, 176, narrow)

    pl.semaphore_wait(barrier, len(peers))

    def other(core):
        return dev(0, 0, 0, core)

    def start(i):
        @pl.when(home)
        def _():
            send_if(
                True, (i, "own"),
                lambda: (w.at[zl, y, whole(i)], w.at[zl, y, whole(i)], other(1 - h)),
            )
            for k in range(2):
                for q, s in ((0, 2), (1, -2)):
                    def make(k=k, q=q, s=s):
                        ref = w.at[zl, y, quarter(i, k, q)]
                        return ref, ref, dev(0, 0, s, k)

                    send_if(True, (i, "zq", q), make, k)

        @pl.when(guest)
        def _():
            for k in range(2):
                for s in (1, -1):
                    def make(k=k, s=s):
                        rows = half(i, k)
                        return mine.at[rows], w.at[zl, y, rows], dev(0, 0, s, k)

                    send_if(False, (i, "z", s), make, k)

    def swap(src, dst, name, wide):
        @pl.when(guest)
        def _():
            for s, part in ((1, pl.ds(0, HT)), (-1, pl.ds(HT, HT))):
                def make(s=s, part=part):
                    at = (part, qcols(0)) if wide else (slice(None), part)
                    return src.at[at], dst.at[at], dev(0, 0, s, p)

                send_if(False, (name, s), make)

    def swapped(dst, name, wide):
        for s, part in ((1, pl.ds(0, HT)), (-1, pl.ds(HT, HT))):
            at = (part, qcols(0)) if wide else (slice(None), part)
            got((name, s), dst.at[at])

    def qcols(k):
        return pl.ds(pl.multiple_of(lax.rem(xx + k + 4, 4) * QD, QD), QD)

    def spread0(dst, name):
        @pl.when(guest)
        def _():
            swapped(dst, name, True)
            for s in (1, -1):
                def make(s=s):
                    ref = dst.at[:, qcols(0)]
                    return ref, ref, dev(s, 0, 0, h)

                send_if(False, (name, "x", s), make)

    def spread1(dst, name):
        @pl.when(guest)
        def _():
            for s, part in ((1, pl.ds(0, HT)), (-1, pl.ds(HT, HT))):
                got((name, "x", s), dst.at[:, qcols(-s)])

                def make(s=s, part=part):
                    ref = dst.at[part, qcols(-s)]
                    return ref, ref, dev(s, 0, 0, h)

                send_if(False, (name, "xf", s), make)

    def spread2(dst, name, load):
        @pl.when(guest)
        def _():
            for s, part in ((1, pl.ds(0, HT)), (-1, pl.ds(HT, HT))):
                got((name, "xf", s), dst.at[part, qcols(2)])

        @pl.when(home)
        def _():
            loads[load].wait()

    def ys(i, c):
        ref = w.at[zi(SIDES[c]), y, half(i, h)]
        if c == 0:
            @pl.when(guest)
            def _():
                got((i, "own"), w.at[zl, y, whole(i)])
        elif c < 3:
            got((i, "z", -SIDES[c]), ref)
        else:
            for q in range(2):
                got((i, "zq", q), w.at[zi(2), y, quarter(i, h, q)])
        for s in (1, -1):
            send((i, "y", c, s), ref, ref, dev(0, s, 0, h))
        if c:
            send((i, "s", c), ref, ref, other(1 - h))

    def yr(i, c, s):
        got((i, "y", c, s), w.at[zi(SIDES[c]), yi(-s), half(i, h)])
        q = 0 if s == 1 else 1
        ref = w.at[zi(SIDES[c]), yi(-s), quarter(i, h, q)]
        send((i, "f", c, s), ref, ref, dev(0, s, 0, h))

    def yt(i, s):
        ref = w.at[:, yi(-s), half(i, h)]
        send((i, "t", s), ref, ref, other(1 - h))

    def yf(i):
        for c in range(4):
            for s, q in ((1, 0), (-1, 1)):
                got((i, "f", c, s), w.at[zi(SIDES[c]), yi(2), quarter(i, h, q)])
        yt(i, 2)

    def last(i):
        for c in range(1, 4):
            got((i, "s", c), w.at[zi(SIDES[c]), y, half(i, 1 - h)])
        for s in (1, -1, 2):
            got((i, "t", s), w.at[:, yi(-s), half(i, 1 - h)])

    def elementwise():
        down_col[...] = jnp.broadcast_to(ds_ref[...], (LANES, FFL)).T

        @pl.when(home)
        def _():
            for k, ref in enumerate((gs_ref, us_ref, ds_ref)):
                scales[k] = jnp.broadcast_to(ref[...], (LANES, FFL)).T
            send_if(True, ("scales",), lambda: (scales, scales, other(1 - h)))
            loads[3].wait()
            loads[4].wait()

        @pl.when(guest)
        def _():
            got(("scales",), scales)
            swapped(gate, "gate", False)
            swapped(up, "up", False)

        def body(i, n):
            rows = span(i, n)
            g = gate[rows, :].astype(F32)
            u = up[rows, :].astype(F32)
            sig = jax.nn.sigmoid(g)
            act = g * sig
            hidden[rows, :] = (act * u).astype(BF16)
            down = scales[2, rows]
            gs = jnp.concatenate([scales[0, rows] * down] * 4, axis=1)
            us = jnp.concatenate([scales[1, rows] * down] * 4, axis=1)
            fg[rows, :] = u * sig * (1.0 + g * (1.0 - sig)) * gs
            fu[rows, :] = act * us

        chunks(FFL, 16, body)

    def down_grads():
        @pl.loop(0, 8)
        def _(k):
            zz, yy = lax.div(k, 2), lax.rem(k, 2) * 2
            cols = pl.ds(pl.multiple_of(k * 256, 256), 256)
            out = jnp.dot(hidden[...], cot[:, cols], preferred_element_type=F32).astype(BF16)
            grad[zz, yy, pl.ds(0, FFL)] = out[:, :LANES]
            grad[zz, yy + 1, pl.ds(0, FFL)] = out[:, LANES:]

    def cotangents():
        @pl.loop(0, 2)
        def _(m):
            cols = pl.ds(pl.multiple_of(m * 256, 256), 256)
            rows = jnp.concatenate(
                [w[i // 4, i % 4, pl.ds(0, FFL)] for i in range(16)], axis=1
            )
            hc = lax.dot_general(
                rows, cot[cols, :], (((1,), (1,)), ((), ())), preferred_element_type=F32
            )
            bc[pl.ds(0, FFL), cols] = (hc * fg[:, cols]).astype(BF16)
            bc[pl.ds(FFL, FFL), cols] = (hc * fu[:, cols]).astype(BF16)

    def gate_up_grads(i):
        @pl.loop(0, 8)
        def _(k):
            zz, yy = lax.div(k, 2), lax.rem(k, 2) * 2
            cols = pl.ds(pl.multiple_of(k * 256, 256), 256)
            lo, n = PIECES[i]
            out = jnp.dot(bc[pl.ds(lo - FFL, n), :], x[:, cols], preferred_element_type=F32).astype(BF16)
            grad[zz, yy, whole(i)] = out[:, :LANES]
            grad[zz, yy + 1, whole(i)] = out[:, LANES:]

    def presum(i):
        for k in (2, 1, -1, 0):
            src = grad.at[:, yi(k), half(i, 1 - h)]
            send((i, "ps", k), src, sib.at[:, yi(k), small(i)], other(1 - h))

    def add(i, k, b, *more):
        lo, size = PIECES[i]

        def body(j, n):
            at = (b, yi(k), span(lo + h * (size // 2) + j, n))
            low = span(lo // 2 + j, n)
            total = grad[at].astype(F32) + sib[b, yi(k), low].astype(F32)
            for ref in more:
                total = total + ref[low].astype(F32)
            grad[at] = total.astype(BF16)

        chunks(size // 2, size // 4, body)

    def part(i, k, b):
        return grad.at[pl.ds(b, 2), yi(k), half(i, h)]

    def got_sib(i, k):
        got((i, "ps", k), sib.at[:, yi(k), small(i)])

    def rs_start(i):
        got_sib(i, 2)
        for b in range(2):
            add(i, 2, b)
        send((i, "r", 0), part(i, 2, 0), r1.at[0, :, small(i)], dev(0, 1, 0, h))
        for b in range(2, 4):
            add(i, 2, b)
        send((i, "r", 1), part(i, 2, 2), r1.at[1, :, small(i)], dev(0, -1, 0, h))
        got_sib(i, 1)
        for b in range(2, 4):
            add(i, 1, b)
        send((i, "r", 2), part(i, 1, 2), r2.at[0, pl.ds(2, 2), small(i)], dev(0, 1, 0, h))
        got_sib(i, -1)
        for b in range(2):
            add(i, -1, b)
        send((i, "r", 3), part(i, -1, 0), r2.at[1, pl.ds(0, 2), small(i)], dev(0, -1, 0, h))

    def rs_plus(i):
        got((i, "r", 0), r1.at[0, :, small(i)])
        for b in range(2):
            add(i, 1, b, r1.at[0, b])
        send((i, "r", 4), part(i, 1, 0), r2.at[0, pl.ds(0, 2), small(i)], dev(0, 1, 0, h))

    def rs_minus(i):
        got((i, "r", 1), r1.at[1, :, small(i)])
        for b in range(2, 4):
            add(i, -1, b, r1.at[1, b - 2])
        send((i, "r", 5), part(i, -1, 2), r2.at[1, pl.ds(2, 2), small(i)], dev(0, -1, 0, h))

    def sum_own(i, k):
        b = zi(k)
        lo, size = PIECES[i]

        def body(j, n):
            rows = span(lo // 2 + j, n)
            total = grad[b, yi(0), span(lo + h * (size // 2) + j, n)].astype(F32)
            total = total + sib[b, yi(0), rows].astype(F32)
            total = total + r2[0, b, rows].astype(F32) + r2[1, b, rows].astype(F32)
            own[b, rows] = total.astype(BF16)

        chunks(size // 2, size // 4, body)

    def rs_own(i):
        got_sib(i, 0)
        got((i, "r", 2), r2.at[0, pl.ds(2, 2), small(i)])
        got((i, "r", 3), r2.at[1, pl.ds(0, 2), small(i)])
        got((i, "r", 4), r2.at[0, pl.ds(0, 2), small(i)])
        got((i, "r", 5), r2.at[1, pl.ds(2, 2), small(i)])
        lo, n = PIECES[i]
        sum_own(i, 2)
        for q, s in ((0, 2), (1, -2)):
            src = own.at[zi(2), pl.ds(lo // 2 + q * (n // 4), n // 4)]
            send((i, "g", q), src, zr.at[q, quarter(i, h, q)], dev(0, 0, s, p), by=h)
        for q, s in ((0, 1), (1, -1)):
            sum_own(i, s)
            src = own.at[zi(s), small(i)]
            send((i, "n", q), src, zr.at[q, half(i, h)], dev(0, 0, s, p), by=h)
        sum_own(i, 0)

        @pl.when(guest)
        def _():
            send_if(
                False, (i, "zs"), lambda: (own.at[zl, small(i)], zs.at[small(i)], other(p))
            )

    def rs_fin(i):
        lo, size = PIECES[i]
        hn, qn = size // 2, size // 4

        @pl.when(home)
        def _():
            for k in range(2):
                for q in range(2):
                    got((i, "g", q), zr.at[q, quarter(i, k, q)], by=k)
            got((i, "zs"), zs.at[small(i)])
            for q in range(2):
                def body(j, n, q=q):
                    low = span(lo // 2 + q * qn + j, n)
                    rows = span(lo + h * hn + q * qn + j, n)
                    total = own[zl, low].astype(F32) + zr[q, rows].astype(F32)
                    final[rows] = total.astype(BF16)
                    rows = span(lo + (1 - h) * hn + q * qn + j, n)
                    total = zs[low].astype(F32) + zr[q, rows].astype(F32)
                    final[rows] = total.astype(BF16)

                chunks(qn, qn, body)

        @pl.when(guest)
        def _():
            for k in range(2):
                for q in range(2):
                    got((i, "n", q), zr.at[q, half(i, k)], by=k)

            def body(j, n):
                rows = span(lo + j, n)
                total = zr[0, rows].astype(F32) + zr[1, rows].astype(F32)
                final[rows] = total.astype(BF16)

            chunks(size, qn, body)

        for q, s in ((0, 2), (1, -2)):
            send((i, "e", q), final.at[half(i, q)], q1.at[q, small(i)], dev(0, 0, s, h))

    def relay(i, q):
        got((i, "e", q), q1.at[q, small(i)])
        s = (2, -2)[q]
        send((i, "k", q), q1.at[q, small(i)], q2.at[half(i, q)], dev(0, 0, s, h))

    def arrive(i):
        for q in range(2):
            got((i, "k", q), q2.at[half(i, q)])
        lo, size = PIECES[i]

        def body(j, n):
            rows = span(lo + j, n)
            total = final[rows].astype(F32) + q2[rows].astype(F32)
            if lo < FFL:
                total = total * down_col[rows]
            out_ref[rows, :] = total

        chunks(size, size // 4, body)

    def partial_inputs():
        @pl.loop(0, 8)
        def _(r):
            t = lax.rem(xx * 2 + r, 8)
            zz, yy = lax.div(t, 2), lax.rem(t, 2) * 2
            rows = pl.ds(FFL, GU)
            both = jnp.concatenate([w[zz, yy, rows], w[zz, yy + 1, rows]], axis=1)
            value = lax.dot_general(
                bc[...], both, (((0,), (0,)), ((), ())), preferred_element_type=F32
            )
            tp_out[lax.div(r, 2), lax.rem(r, 2)] = value.astype(BF16)

        for k, s in ((0, 1), (1, -1)):
            send(("p", k), tp_out.at[2, :, tokens[k]], xr1.at[k], dev(s, 0, 0, h))
        send(("p", 2), tp_out.at[1, :, tokens[1]], xr2.at[0, :, tokens[1]], dev(1, 0, 0, h))
        send(("p", 3), tp_out.at[3, :, tokens[0]], xr2.at[1, :, tokens[0]], dev(-1, 0, 0, h))

    tokens = (pl.ds(0, HT), pl.ds(HT, HT))

    def partial_on(k):
        s = (1, -1)[k]
        got(("p", k), xr1.at[k])
        for core in range(2):
            def body(j, n, core=core):
                at = (s % 4, core, span(k * HT + j, n))
                total = tp_out[at].astype(F32) + xr1[k, core, span(j, n)].astype(F32)
                tp_out[at] = total.astype(BF16)

            chunks(HT, 128, body)
        send(
            ("p", 4 + k), tp_out.at[s % 4, :, tokens[k]], xr2.at[k, :, tokens[k]],
            dev(s, 0, 0, h),
        )

    def partial_sum():
        got(("p", 2), xr2.at[0, :, tokens[1]])
        got(("p", 3), xr2.at[1, :, tokens[0]])
        got(("p", 4), xr2.at[0, :, tokens[0]])
        got(("p", 5), xr2.at[1, :, tokens[1]])
        for core in range(2):
            def body(j, n, core=core):
                rows = span(j, n)
                total = tp_out[0, core, rows].astype(F32) + xr2[0, core, rows].astype(F32)
                total = total + xr2[1, core, rows].astype(F32)
                tp_out[0, core, rows] = total.astype(BF16)

            chunks(TOK, 128, body)

        @pl.when(home)
        def _():
            send_if(
                True, ("h",), lambda: (tp_out.at[0, 1 - h], from_home, other(1 - h))
            )

            def keep(j, n):
                from_home[span(j, n)] = tp_out[0, h, span(j, n)]

            chunks(TOK, 128, keep)

        @pl.when(guest)
        def _():
            for core in range(2):
                for s, rows in ((-1, tokens[0]), (1, tokens[1])):
                    def make(core=core, s=s, rows=rows):
                        return tp_out.at[0, core, rows], from_guest.at[rows], dev(0, 0, s, core)

                    send_if(False, ("g", s), make, core)

    def input_grad():
        @pl.when(guest)
        def _():
            got(("h",), from_home)

        for s, rows in ((-1, tokens[0]), (1, tokens[1])):
            got(("g", s), from_guest.at[rows])

        def body(j, n):
            rows = span(j, n)
            total = from_home[rows].astype(F32) + from_guest[rows].astype(F32)
            oi_ref[rows, :] = total.astype(BF16)

        chunks(TOK, 128, body)

    work = {
        "st": start, "ys": ys, "yr": yr, "yt": yt, "yf": yf, "last": last,
        "ew": elementwise, "down": down_grads, "hc": cotangents, "gu": gate_up_grads,
        "part": partial_inputs, "p": partial_on, "psum": partial_sum, "tp": input_grad, "ps": presum, "rs": rs_start,
        "r+": rs_plus, "r-": rs_minus, "own": rs_own, "fin": rs_fin, "y": relay, "arr": arrive,
        "sgu": lambda: (swap(gate_hbm, gate, "gate", False), swap(up_hbm, up, "up", False)),
        "sc": lambda: swap(cot_hbm, cot, "cot", True),
        "sx": lambda: swap(x_hbm, x, "x", True),
        "c0": lambda: spread0(cot, "cot"), "c1": lambda: spread1(cot, "cot"),
        "c2": lambda: spread2(cot, "cot", 5),
        "x0": lambda: spread0(x, "x"), "x1": lambda: spread1(x, "x"),
        "x2": lambda: spread2(x, "x", 6),
    }
    for step in ORDER:
        name, *args = step.split(" ")
        work[name](*(int(a) for a in args))
    assert len(send_ids) <= SEMS and sum(recv_sizes) <= SEMS, (len(send_ids), sum(recv_sizes))

    for cond in (None, True, False):
        def drain(cond=cond):
            for c, make, s in sends:
                if c is cond:
                    src, dst, peer = make()
                    remote(src, dst, s, 0, peer).wait_send()

        if cond is None:
            drain()
        else:
            pl.when(home if cond else guest)(drain)


SEMS = 288


def hand_out(oi_in, all_in, oi_out, og_out, ou_out, od_out, oi, grads, in_sem, out_sem):
    pieces = [(oi_in, oi, oi_out)]
    for k, ref in enumerate((od_out, og_out, ou_out)):
        rows = pl.ds(k * FFL, FFL)
        pieces.append((all_in.at[rows], grads.at[rows], ref))
    copies = []
    for k, (src, mid, dst) in enumerate(pieces):
        first = pltpu.make_async_copy(src, mid, in_sem.at[k])
        first.start()
        copies.append((first, pltpu.make_async_copy(mid, dst, out_sem.at[k])))
    for first, second in copies:
        first.wait()
        second.start()
    for _, second in copies:
        second.wait()


def local(
    inputs, cotangent, gate_pre, up_pre, gate_weight, up_weight, down_weight,
    gate_scale, up_scale, down_scale,
):
    hbm = pl.BlockSpec(memory_space=pl.ANY)
    vmem = pl.BlockSpec(memory_space=pltpu.VMEM)
    sem = pltpu.SemaphoreType.DMA
    half = ALL // 2
    oi, out = pl.pallas_call(
        kernel,
        out_shape=(
            jax.ShapeDtypeStruct((TOK, 256), BF16),
            jax.ShapeDtypeStruct((ALL, LANES), F32),
        ),
        in_specs=[hbm] * 7 + [vmem] * 3,
        out_specs=(vmem,) * 2,
        scratch_shapes=[
            pltpu.VMEM((TOK, D), BF16),
            pltpu.VMEM((TOK, D), BF16),
            pltpu.VMEM((FFL, TOK), BF16),
            pltpu.VMEM((FFL, TOK), BF16),
            pltpu.VMEM((ALL, LANES), F32),
            pltpu.VMEM((3, FFL, LANES), F32),
            pltpu.VMEM((FFL, LANES), F32),
            pltpu.VMEM((FFL, TOK), BF16),
            pltpu.VMEM((FFL, TOK), F32),
            pltpu.VMEM((FFL, TOK), F32),
            pltpu.VMEM((GU, TOK), BF16),
            pltpu.VMEM((4, 4, ALL, LANES), BF16),
            pltpu.VMEM((ALL, LANES), BF16),
            pltpu.VMEM((4, 4, ALL, LANES), BF16),
            pltpu.VMEM((4, 4, half, LANES), BF16),
            pltpu.VMEM((2, 2, half, LANES), BF16),
            pltpu.VMEM((2, 4, half, LANES), BF16),
            pltpu.VMEM((4, half, LANES), BF16),
            pltpu.VMEM((2, ALL, LANES), BF16),
            pltpu.VMEM((half, LANES), BF16),
            pltpu.VMEM((ALL, LANES), BF16),
            pltpu.VMEM((2, half, LANES), BF16),
            pltpu.VMEM((ALL, LANES), BF16),
            pltpu.VMEM((4, 2, TOK, 256), BF16),
            pltpu.VMEM((2, 2, HT, 256), BF16),
            pltpu.VMEM((2, 2, TOK, 256), BF16),
            pltpu.VMEM((TOK, 256), BF16),
            pltpu.VMEM((TOK, 256), BF16),
            sem((7,)),
            sem((SEMS,)),
            sem((SEMS,)),
        ],
        compiler_params=pltpu.CompilerParams(
            collective_id=0, has_side_effects=True, vmem_limit_bytes=58 * 1024 * 1024
        ),
    )(
        inputs, cotangent, gate_pre.T, up_pre.T,
        down_weight.T, gate_weight.T, up_weight.T, gate_scale, up_scale, down_scale,
    )
    oi, og, ou, od = pl.pallas_call(
        hand_out,
        out_shape=(
            jax.ShapeDtypeStruct((TOK, 256), BF16),
            jax.ShapeDtypeStruct((FFL, LANES), F32),
            jax.ShapeDtypeStruct((FFL, LANES), F32),
            jax.ShapeDtypeStruct((FFL, LANES), F32),
        ),
        in_specs=[hbm] * 2,
        out_specs=(hbm,) * 4,
        scratch_shapes=[
            pltpu.VMEM((TOK, 256), BF16), pltpu.VMEM((ALL, LANES), F32), sem((4,)), sem((4,)),
        ],
        compiler_params=pltpu.CompilerParams(vmem_limit_bytes=60 * 1024 * 1024),
    )(oi, out)
    return oi, og.T, ou.T, od.T


def solution(mesh):
    rows = ("rep", "fs")
    in_specs = (
        P(rows, None), P(rows, None), P(rows, "tp"), P(rows, "tp"),
        P("fs", "tp"), P("fs", "tp"), P("fs", "tp"),
        P(None, "tp"), P(None, "tp"), P(None, "tp"),
    )
    out_specs = (P(rows, "tp"), P("fs", "tp"), P("fs", "tp"), P("fs", "tp"))
    return jax.shard_map(local, mesh=mesh, in_specs=in_specs, out_specs=out_specs, check_vma=False)
```

```python
import jax
import jax.numpy as jnp
from jax import lax
from jax.experimental import pallas as pl
from jax.experimental.pallas import tpu as pltpu
from jax.sharding import PartitionSpec as P

MESH = pl.DeviceIdType.MESH
F32 = jnp.float32
BF16 = jnp.bfloat16
LANES = 128
TOK = 512
HT = TOK // 2
D = 2048
QD = D // 4
FFL = 704
GU = 2 * FFL
ALL = 3 * FFL
SIDES = (0, -1, 1, 2)

PIECES = ((0, 704), (704, 704), (1408, 704))
ORDER = (
    "st 2", "sc", "st 0", "ys 0 0", "ys 2 0", "st 1", "ys 1 0", "ys 2 2", "ys 2 1", "ys 0 3",
    "c0", "ys 2 3", "sgu", "sx", "yr 0 0 -1", "ys 1 3", "ys 0 1", "ys 0 2", "ys 1 1", "ys 1 2",
    "c1", "yr 0 1 -1", "yr 0 3 1", "yr 0 2 1", "ew", "yr 2 2 1", "x0", "yr 0 3 -1",
    "yr 2 3 -1", "yr 2 2 -1", "yr 0 2 -1", "yr 2 0 -1", "yr 1 0 -1", "yr 2 1 1", "c2",
    "yr 0 0 1", "yr 0 1 1", "yt 0 -1", "yr 1 2 1", "yr 1 3 -1", "yr 1 1 -1", "yr 1 3 1",
    "yr 1 1 1", "yr 1 2 -1", "yr 1 0 1", "yt 0 1", "down", "yr 2 0 1", "yr 2 1 -1", "ps 0",
    "yf 0", "yt 1 1", "rs 0", "yt 2 -1", "x1", "yr 2 3 1", "last 0", "yf 1", "hc", "x2",
    "r+ 0", "yt 2 1", "r- 0", "gu 1", "yf 2", "ps 1", "rs 1", "own 0", "gu 2", "yt 1 -1",
    "last 2", "r- 1", "ps 2", "r+ 1", "fin 0", "rs 2", "own 1", "last 1", "part", "y 0 1",
    "y 0 0", "fin 1", "r- 2", "r+ 2", "own 2", "y 1 1", "p 1", "y 1 0", "p 0", "fin 2", "psum",
    "y 2 1", "y 2 0", "tp", "arr 1", "arr 0", "arr 2",
)

def kernel(
    x_hbm, cot_hbm, gate_hbm, up_hbm, wd_hbm, wg_hbm, wu_hbm, gs_ref, us_ref, ds_ref,
    oi_hbm, out_hbm,
    x, cot, gate, up, w32, scales, down_col, hidden, fg, fu, bc,
    w, mine, grad, sib, r1, r2, own, zr, zs, final, q1, q2,
    tp_out, xr1, xr2, from_home, from_guest,
    oi_ref, out_ref, local_sem, send_sem, recv_sem,
):
    rep = lax.axis_index("rep")
    fs = lax.axis_index("fs")
    tp = lax.axis_index("tp")
    y = lax.rem(fs, 4)
    zl = lax.div(fs, 4)
    z = rep * 4 + zl
    xx = lax.div(tp, 2)
    h = lax.rem(tp, 2)
    p = lax.rem(zl, 2)
    home = h == p
    guest = h != p

    def dev(dx, dy, dz, core):
        nx = lax.rem(xx + dx + 4, 4)
        ny = lax.rem(y + dy + 4, 4)
        nz = lax.rem(z + dz + 8, 8)
        return (lax.div(nz, 4), lax.rem(nz, 4) * 4 + ny, nx * 2 + core)

    def yi(k):
        return lax.rem(y + k + 4, 4)

    def zi(k):
        return lax.rem(zl + k + 4, 4)

    def chunks(n, size, fn):
        if n == size:
            fn(0, size)
            return

        @pl.loop(0, n // size)
        def _(i):
            fn(i * size, size)

    def span(start, size):
        return pl.ds(start if isinstance(start, int) else pl.multiple_of(start, 16), size)

    def whole(i):
        lo, n = PIECES[i]
        return pl.ds(lo, n)

    def half(i, k):
        lo, n = PIECES[i]
        return pl.ds(pl.multiple_of(lo + k * (n // 2), 16), n // 2)

    def quarter(i, k, q):
        lo, n = PIECES[i]
        return pl.ds(pl.multiple_of(lo + k * (n // 2) + q * (n // 4), 16), n // 4)

    def small(i):
        lo, n = PIECES[i]
        return pl.ds(lo // 2, n // 2)

    send_ids, recv_ids = {}, {}
    sends = []

    def remote(src, dst, s, r, peer):
        return pltpu.make_async_remote_copy(
            src_ref=src, dst_ref=dst, send_sem=send_sem.at[s], recv_sem=recv_sem.at[r],
            device_id=peer, device_id_type=MESH,
        )

    def rid(name, spread):
        key = name if spread is None else (*name, "by")
        if key not in recv_ids:
            recv_ids[key] = sum(recv_sizes)
            recv_sizes.append(1 if spread is None else 2)
        return recv_ids[key] if spread is None else recv_ids[key] + spread

    recv_sizes = []

    def send(name, src, dst, peer, tag="", by=None):
        s = send_ids.setdefault((*name, tag), len(send_ids))
        remote(src, dst, s, rid(name, by), peer).start()
        sends.append((None, lambda: (src, dst, peer), s))

    def send_if(cond, name, make, tag=""):
        s = send_ids.setdefault((*name, tag), len(send_ids))
        src, dst, peer = make()
        remote(src, dst, s, rid(name, None), peer).start()
        sends.append((cond, make, s))

    def got(name, dst, by=None):
        remote(dst, dst, 0, rid(name, by), dev(0, 1, 0, h)).wait_recv()

    loads = []
    for k, (src, dst) in enumerate(
        (
            (wd_hbm, w32.at[pl.ds(0, FFL)]),
            (wg_hbm, w32.at[pl.ds(FFL, FFL)]),
            (wu_hbm, w32.at[pl.ds(GU, FFL)]),
            (gate_hbm, gate),
            (up_hbm, up),
            (cot_hbm, cot),
            (x_hbm, x),
        )
    ):
        loads.append(pltpu.make_async_copy(src, dst, local_sem.at[k]))
    for k in range(3):
        loads[k].start()

    barrier = pltpu.get_barrier_semaphore()
    peers = [dev(0, 1, 0, h), dev(0, -1, 0, h), dev(1, 0, 0, h), dev(-1, 0, 0, h)]
    for core in range(2):
        peers += [dev(0, 0, k, core) for k in (1, -1, 2, -2)]
    peers.append(dev(0, 0, 0, 1 - h))
    for peer in peers:
        pl.semaphore_signal(barrier, inc=1, device_id=peer, device_id_type=MESH)

    @pl.when(home)
    def _():
        for k in range(3, 7):
            loads[k].start()

    for k in range(3):
        loads[k].wait()

    @pl.when(home)
    def _():
        def narrow(i, n):
            w[zl, y, span(i, n)] = w32[span(i, n)].astype(BF16)

        chunks(ALL, 176, narrow)

    @pl.when(guest)
    def _():
        def narrow(i, n):
            mine[span(i, n)] = w32[span(i, n)].astype(BF16)

        chunks(ALL, 176, narrow)

    pl.semaphore_wait(barrier, len(peers))

    def other(core):
        return dev(0, 0, 0, core)

    def start(i):
        @pl.when(home)
        def _():
            send_if(
                True, (i, "own"),
                lambda: (w.at[zl, y, whole(i)], w.at[zl, y, whole(i)], other(1 - h)),
            )
            for k in range(2):
                for q, s in ((0, 2), (1, -2)):
                    def make(k=k, q=q, s=s):
                        ref = w.at[zl, y, quarter(i, k, q)]
                        return ref, ref, dev(0, 0, s, k)

                    send_if(True, (i, "zq", q), make, k)

        @pl.when(guest)
        def _():
            for k in range(2):
                for s in (1, -1):
                    def make(k=k, s=s):
                        rows = half(i, k)
                        return mine.at[rows], w.at[zl, y, rows], dev(0, 0, s, k)

                    send_if(False, (i, "z", s), make, k)

    def swap(src, dst, name, wide):
        @pl.when(guest)
        def _():
            for s, part in ((1, pl.ds(0, HT)), (-1, pl.ds(HT, HT))):
                def make(s=s, part=part):
                    at = (part, qcols(0)) if wide else (slice(None), part)
                    return src.at[at], dst.at[at], dev(0, 0, s, p)

                send_if(False, (name, s), make)

    def swapped(dst, name, wide):
        for s, part in ((1, pl.ds(0, HT)), (-1, pl.ds(HT, HT))):
            at = (part, qcols(0)) if wide else (slice(None), part)
            got((name, s), dst.at[at])

    def qcols(k):
        return pl.ds(pl.multiple_of(lax.rem(xx + k + 4, 4) * QD, QD), QD)

    def spread0(dst, name):
        @pl.when(guest)
        def _():
            swapped(dst, name, True)
            for s in (1, -1):
                def make(s=s):
                    ref = dst.at[:, qcols(0)]
                    return ref, ref, dev(s, 0, 0, h)

                send_if(False, (name, "x", s), make)

    def spread1(dst, name):
        @pl.when(guest)
        def _():
            for s, part in ((1, pl.ds(0, HT)), (-1, pl.ds(HT, HT))):
                got((name, "x", s), dst.at[:, qcols(-s)])

                def make(s=s, part=part):
                    ref = dst.at[part, qcols(-s)]
                    return ref, ref, dev(s, 0, 0, h)

                send_if(False, (name, "xf", s), make)

    def spread2(dst, name, load):
        @pl.when(guest)
        def _():
            for s, part in ((1, pl.ds(0, HT)), (-1, pl.ds(HT, HT))):
                got((name, "xf", s), dst.at[part, qcols(2)])

        @pl.when(home)
        def _():
            loads[load].wait()

    def ys(i, c):
        ref = w.at[zi(SIDES[c]), y, half(i, h)]
        if c == 0:
            @pl.when(guest)
            def _():
                got((i, "own"), w.at[zl, y, whole(i)])
        elif c < 3:
            got((i, "z", -SIDES[c]), ref)
        else:
            for q in range(2):
                got((i, "zq", q), w.at[zi(2), y, quarter(i, h, q)])
        for s in (1, -1):
            send((i, "y", c, s), ref, ref, dev(0, s, 0, h))
        if c:
            send((i, "s", c), ref, ref, other(1 - h))

    def yr(i, c, s):
        got((i, "y", c, s), w.at[zi(SIDES[c]), yi(-s), half(i, h)])
        q = 0 if s == 1 else 1
        ref = w.at[zi(SIDES[c]), yi(-s), quarter(i, h, q)]
        send((i, "f", c, s), ref, ref, dev(0, s, 0, h))

    def yt(i, s):
        ref = w.at[:, yi(-s), half(i, h)]
        send((i, "t", s), ref, ref, other(1 - h))

    def yf(i):
        for c in range(4):
            for s, q in ((1, 0), (-1, 1)):
                got((i, "f", c, s), w.at[zi(SIDES[c]), yi(2), quarter(i, h, q)])
        yt(i, 2)

    def last(i):
        for c in range(1, 4):
            got((i, "s", c), w.at[zi(SIDES[c]), y, half(i, 1 - h)])
        for s in (1, -1, 2):
            got((i, "t", s), w.at[:, yi(-s), half(i, 1 - h)])

    def elementwise():
        down_col[...] = jnp.broadcast_to(ds_ref[...], (LANES, FFL)).T

        @pl.when(home)
        def _():
            for k, ref in enumerate((gs_ref, us_ref, ds_ref)):
                scales[k] = jnp.broadcast_to(ref[...], (LANES, FFL)).T
            send_if(True, ("scales",), lambda: (scales, scales, other(1 - h)))
            loads[3].wait()
            loads[4].wait()

        @pl.when(guest)
        def _():
            got(("scales",), scales)
            swapped(gate, "gate", False)
            swapped(up, "up", False)

        def body(i, n):
            rows = span(i, n)
            g = gate[rows, :].astype(F32)
            u = up[rows, :].astype(F32)
            sig = jax.nn.sigmoid(g)
            act = g * sig
            hidden[rows, :] = (act * u).astype(BF16)
            down = scales[2, rows]
            gs = jnp.concatenate([scales[0, rows] * down] * 4, axis=1)
            us = jnp.concatenate([scales[1, rows] * down] * 4, axis=1)
            fg[rows, :] = u * sig * (1.0 + g * (1.0 - sig)) * gs
            fu[rows, :] = act * us

        chunks(FFL, 16, body)

    def down_grads():
        @pl.loop(0, 8)
        def _(k):
            zz, yy = lax.div(k, 2), lax.rem(k, 2) * 2
            cols = pl.ds(pl.multiple_of(k * 256, 256), 256)
            out = jnp.dot(hidden[...], cot[:, cols], preferred_element_type=F32).astype(BF16)
            grad[zz, yy, pl.ds(0, FFL)] = out[:, :LANES]
            grad[zz, yy + 1, pl.ds(0, FFL)] = out[:, LANES:]

    def cotangents():
        @pl.loop(0, 2)
        def _(m):
            cols = pl.ds(pl.multiple_of(m * 256, 256), 256)
            rows = jnp.concatenate(
                [w[i // 4, i % 4, pl.ds(0, FFL)] for i in range(16)], axis=1
            )
            hc = lax.dot_general(
                rows, cot[cols, :], (((1,), (1,)), ((), ())), preferred_element_type=F32
            )
            bc[pl.ds(0, FFL), cols] = (hc * fg[:, cols]).astype(BF16)
            bc[pl.ds(FFL, FFL), cols] = (hc * fu[:, cols]).astype(BF16)

    def gate_up_grads(i):
        @pl.loop(0, 8)
        def _(k):
            zz, yy = lax.div(k, 2), lax.rem(k, 2) * 2
            cols = pl.ds(pl.multiple_of(k * 256, 256), 256)
            lo, n = PIECES[i]
            out = jnp.dot(bc[pl.ds(lo - FFL, n), :], x[:, cols], preferred_element_type=F32).astype(BF16)
            grad[zz, yy, whole(i)] = out[:, :LANES]
            grad[zz, yy + 1, whole(i)] = out[:, LANES:]

    def presum(i):
        for k in (2, 1, -1, 0):
            src = grad.at[:, yi(k), half(i, 1 - h)]
            send((i, "ps", k), src, sib.at[:, yi(k), small(i)], other(1 - h))

    def add(i, k, b, *more):
        lo, size = PIECES[i]

        def body(j, n):
            at = (b, yi(k), span(lo + h * (size // 2) + j, n))
            low = span(lo // 2 + j, n)
            total = grad[at].astype(F32) + sib[b, yi(k), low].astype(F32)
            for ref in more:
                total = total + ref[low].astype(F32)
            grad[at] = total.astype(BF16)

        chunks(size // 2, size // 4, body)

    def part(i, k, b):
        return grad.at[pl.ds(b, 2), yi(k), half(i, h)]

    def got_sib(i, k):
        got((i, "ps", k), sib.at[:, yi(k), small(i)])

    def rs_start(i):
        got_sib(i, 2)
        for b in range(2):
            add(i, 2, b)
        send((i, "r", 0), part(i, 2, 0), r1.at[0, :, small(i)], dev(0, 1, 0, h))
        for b in range(2, 4):
            add(i, 2, b)
        send((i, "r", 1), part(i, 2, 2), r1.at[1, :, small(i)], dev(0, -1, 0, h))
        got_sib(i, 1)
        for b in range(2, 4):
            add(i, 1, b)
        send((i, "r", 2), part(i, 1, 2), r2.at[0, pl.ds(2, 2), small(i)], dev(0, 1, 0, h))
        got_sib(i, -1)
        for b in range(2):
            add(i, -1, b)
        send((i, "r", 3), part(i, -1, 0), r2.at[1, pl.ds(0, 2), small(i)], dev(0, -1, 0, h))

    def rs_plus(i):
        got((i, "r", 0), r1.at[0, :, small(i)])
        for b in range(2):
            add(i, 1, b, r1.at[0, b])
        send((i, "r", 4), part(i, 1, 0), r2.at[0, pl.ds(0, 2), small(i)], dev(0, 1, 0, h))

    def rs_minus(i):
        got((i, "r", 1), r1.at[1, :, small(i)])
        for b in range(2, 4):
            add(i, -1, b, r1.at[1, b - 2])
        send((i, "r", 5), part(i, -1, 2), r2.at[1, pl.ds(2, 2), small(i)], dev(0, -1, 0, h))

    def sum_own(i, k):
        b = zi(k)
        lo, size = PIECES[i]

        def body(j, n):
            rows = span(lo // 2 + j, n)
            total = grad[b, yi(0), span(lo + h * (size // 2) + j, n)].astype(F32)
            total = total + sib[b, yi(0), rows].astype(F32)
            total = total + r2[0, b, rows].astype(F32) + r2[1, b, rows].astype(F32)
            own[b, rows] = total.astype(BF16)

        chunks(size // 2, size // 4, body)

    def rs_own(i):
        got_sib(i, 0)
        got((i, "r", 2), r2.at[0, pl.ds(2, 2), small(i)])
        got((i, "r", 3), r2.at[1, pl.ds(0, 2), small(i)])
        got((i, "r", 4), r2.at[0, pl.ds(0, 2), small(i)])
        got((i, "r", 5), r2.at[1, pl.ds(2, 2), small(i)])
        lo, n = PIECES[i]
        sum_own(i, 2)
        for q, s in ((0, 2), (1, -2)):
            src = own.at[zi(2), pl.ds(lo // 2 + q * (n // 4), n // 4)]
            send((i, "g", q), src, zr.at[q, quarter(i, h, q)], dev(0, 0, s, p), by=h)
        for q, s in ((0, 1), (1, -1)):
            sum_own(i, s)
            src = own.at[zi(s), small(i)]
            send((i, "n", q), src, zr.at[q, half(i, h)], dev(0, 0, s, p), by=h)
        sum_own(i, 0)

        @pl.when(guest)
        def _():
            send_if(
                False, (i, "zs"), lambda: (own.at[zl, small(i)], zs.at[small(i)], other(p))
            )

    def rs_fin(i):
        lo, size = PIECES[i]
        hn, qn = size // 2, size // 4

        @pl.when(home)
        def _():
            for k in range(2):
                for q in range(2):
                    got((i, "g", q), zr.at[q, quarter(i, k, q)], by=k)
            got((i, "zs"), zs.at[small(i)])
            for q in range(2):
                def body(j, n, q=q):
                    low = span(lo // 2 + q * qn + j, n)
                    rows = span(lo + h * hn + q * qn + j, n)
                    total = own[zl, low].astype(F32) + zr[q, rows].astype(F32)
                    final[rows] = total.astype(BF16)
                    rows = span(lo + (1 - h) * hn + q * qn + j, n)
                    total = zs[low].astype(F32) + zr[q, rows].astype(F32)
                    final[rows] = total.astype(BF16)

                chunks(qn, qn, body)

        @pl.when(guest)
        def _():
            for k in range(2):
                for q in range(2):
                    got((i, "n", q), zr.at[q, half(i, k)], by=k)

            def body(j, n):
                rows = span(lo + j, n)
                total = zr[0, rows].astype(F32) + zr[1, rows].astype(F32)
                final[rows] = total.astype(BF16)

            chunks(size, qn, body)

        for q, s in ((0, 2), (1, -2)):
            send((i, "e", q), final.at[half(i, q)], q1.at[q, small(i)], dev(0, 0, s, h))

    def relay(i, q):
        got((i, "e", q), q1.at[q, small(i)])
        s = (2, -2)[q]
        send((i, "k", q), q1.at[q, small(i)], q2.at[half(i, q)], dev(0, 0, s, h))

    def arrive(i):
        for q in range(2):
            got((i, "k", q), q2.at[half(i, q)])
        lo, size = PIECES[i]

        def body(j, n):
            rows = span(lo + j, n)
            total = final[rows].astype(F32) + q2[rows].astype(F32)
            if lo < FFL:
                total = total * down_col[rows]
            out_ref[rows, :] = total

        chunks(size, size // 4, body)
        leave(out_ref.at[whole(i)], out_hbm.at[whole(i)], 7 + i)

    leaving = []

    def leave(src, dst, k):
        leaving.append(pltpu.make_async_copy(src, dst, local_sem.at[k]))
        leaving[-1].start()

    def partial_inputs():
        @pl.loop(0, 8)
        def _(r):
            t = lax.rem(xx * 2 + r, 8)
            zz, yy = lax.div(t, 2), lax.rem(t, 2) * 2
            rows = pl.ds(FFL, GU)
            both = jnp.concatenate([w[zz, yy, rows], w[zz, yy + 1, rows]], axis=1)
            value = lax.dot_general(
                bc[...], both, (((0,), (0,)), ((), ())), preferred_element_type=F32
            )
            tp_out[lax.div(r, 2), lax.rem(r, 2)] = value.astype(BF16)

        for k, s in ((0, 1), (1, -1)):
            send(("p", k), tp_out.at[2, :, tokens[k]], xr1.at[k], dev(s, 0, 0, h))
        send(("p", 2), tp_out.at[1, :, tokens[1]], xr2.at[0, :, tokens[1]], dev(1, 0, 0, h))
        send(("p", 3), tp_out.at[3, :, tokens[0]], xr2.at[1, :, tokens[0]], dev(-1, 0, 0, h))

    tokens = (pl.ds(0, HT), pl.ds(HT, HT))

    def partial_on(k):
        s = (1, -1)[k]
        got(("p", k), xr1.at[k])
        for core in range(2):
            def body(j, n, core=core):
                at = (s % 4, core, span(k * HT + j, n))
                total = tp_out[at].astype(F32) + xr1[k, core, span(j, n)].astype(F32)
                tp_out[at] = total.astype(BF16)

            chunks(HT, 128, body)
        send(
            ("p", 4 + k), tp_out.at[s % 4, :, tokens[k]], xr2.at[k, :, tokens[k]],
            dev(s, 0, 0, h),
        )

    def partial_sum():
        got(("p", 2), xr2.at[0, :, tokens[1]])
        got(("p", 3), xr2.at[1, :, tokens[0]])
        got(("p", 4), xr2.at[0, :, tokens[0]])
        got(("p", 5), xr2.at[1, :, tokens[1]])
        for core in range(2):
            def body(j, n, core=core):
                rows = span(j, n)
                total = tp_out[0, core, rows].astype(F32) + xr2[0, core, rows].astype(F32)
                total = total + xr2[1, core, rows].astype(F32)
                tp_out[0, core, rows] = total.astype(BF16)

            chunks(TOK, 128, body)

        @pl.when(home)
        def _():
            send_if(
                True, ("h",), lambda: (tp_out.at[0, 1 - h], from_home, other(1 - h))
            )

            def keep(j, n):
                from_home[span(j, n)] = tp_out[0, h, span(j, n)]

            chunks(TOK, 128, keep)

        @pl.when(guest)
        def _():
            for core in range(2):
                for s, rows in ((-1, tokens[0]), (1, tokens[1])):
                    def make(core=core, s=s, rows=rows):
                        return tp_out.at[0, core, rows], from_guest.at[rows], dev(0, 0, s, core)

                    send_if(False, ("g", s), make, core)

    def input_grad():
        @pl.when(guest)
        def _():
            got(("h",), from_home)

        for s, rows in ((-1, tokens[0]), (1, tokens[1])):
            got(("g", s), from_guest.at[rows])

        def body(j, n):
            rows = span(j, n)
            total = from_home[rows].astype(F32) + from_guest[rows].astype(F32)
            oi_ref[rows, :] = total.astype(BF16)

        chunks(TOK, 128, body)
        leave(oi_ref, oi_hbm, 10)

    work = {
        "st": start, "ys": ys, "yr": yr, "yt": yt, "yf": yf, "last": last,
        "ew": elementwise, "down": down_grads, "hc": cotangents, "gu": gate_up_grads,
        "part": partial_inputs, "p": partial_on, "psum": partial_sum, "tp": input_grad, "ps": presum, "rs": rs_start,
        "r+": rs_plus, "r-": rs_minus, "own": rs_own, "fin": rs_fin, "y": relay, "arr": arrive,
        "sgu": lambda: (swap(gate_hbm, gate, "gate", False), swap(up_hbm, up, "up", False)),
        "sc": lambda: swap(cot_hbm, cot, "cot", True),
        "sx": lambda: swap(x_hbm, x, "x", True),
        "c0": lambda: spread0(cot, "cot"), "c1": lambda: spread1(cot, "cot"),
        "c2": lambda: spread2(cot, "cot", 5),
        "x0": lambda: spread0(x, "x"), "x1": lambda: spread1(x, "x"),
        "x2": lambda: spread2(x, "x", 6),
    }
    for step in ORDER:
        name, *args = step.split(" ")
        work[name](*(int(a) for a in args))
    assert len(send_ids) <= SEMS and sum(recv_sizes) <= SEMS, (len(send_ids), sum(recv_sizes))

    for c in leaving:
        c.wait()

    for cond in (None, True, False):
        def drain(cond=cond):
            for c, make, s in sends:
                if c is cond:
                    src, dst, peer = make()
                    remote(src, dst, s, 0, peer).wait_send()

        if cond is None:
            drain()
        else:
            pl.when(home if cond else guest)(drain)


SEMS = 288


def hand_out(oi_in, all_in, oi_out, og_out, ou_out, od_out, oi, grads, in_sem, out_sem):
    pieces = [(oi_in, oi, oi_out)]
    for k, ref in enumerate((od_out, og_out, ou_out)):
        rows = pl.ds(k * FFL, FFL)
        pieces.append((all_in.at[rows], grads.at[rows], ref))
    copies = []
    for k, (src, mid, dst) in enumerate(pieces):
        first = pltpu.make_async_copy(src, mid, in_sem.at[k])
        first.start()
        copies.append((first, pltpu.make_async_copy(mid, dst, out_sem.at[k])))
    for first, second in copies:
        first.wait()
        second.start()
    for _, second in copies:
        second.wait()


def local(
    inputs, cotangent, gate_pre, up_pre, gate_weight, up_weight, down_weight,
    gate_scale, up_scale, down_scale,
):
    hbm = pl.BlockSpec(memory_space=pl.ANY)
    vmem = pl.BlockSpec(memory_space=pltpu.VMEM)
    sem = pltpu.SemaphoreType.DMA
    half = ALL // 2
    oi, out = pl.pallas_call(
        kernel,
        out_shape=(
            jax.ShapeDtypeStruct((TOK, 256), BF16),
            jax.ShapeDtypeStruct((ALL, LANES), F32),
        ),
        in_specs=[hbm] * 7 + [vmem] * 3,
        out_specs=(hbm,) * 2,
        scratch_shapes=[
            pltpu.VMEM((TOK, D), BF16),
            pltpu.VMEM((TOK, D), BF16),
            pltpu.VMEM((FFL, TOK), BF16),
            pltpu.VMEM((FFL, TOK), BF16),
            pltpu.VMEM((ALL, LANES), F32),
            pltpu.VMEM((3, FFL, LANES), F32),
            pltpu.VMEM((FFL, LANES), F32),
            pltpu.VMEM((FFL, TOK), BF16),
            pltpu.VMEM((FFL, TOK), F32),
            pltpu.VMEM((FFL, TOK), F32),
            pltpu.VMEM((GU, TOK), BF16),
            pltpu.VMEM((4, 4, ALL, LANES), BF16),
            pltpu.VMEM((ALL, LANES), BF16),
            pltpu.VMEM((4, 4, ALL, LANES), BF16),
            pltpu.VMEM((4, 4, half, LANES), BF16),
            pltpu.VMEM((2, 2, half, LANES), BF16),
            pltpu.VMEM((2, 4, half, LANES), BF16),
            pltpu.VMEM((4, half, LANES), BF16),
            pltpu.VMEM((2, ALL, LANES), BF16),
            pltpu.VMEM((half, LANES), BF16),
            pltpu.VMEM((ALL, LANES), BF16),
            pltpu.VMEM((2, half, LANES), BF16),
            pltpu.VMEM((ALL, LANES), BF16),
            pltpu.VMEM((4, 2, TOK, 256), BF16),
            pltpu.VMEM((2, 2, HT, 256), BF16),
            pltpu.VMEM((2, 2, TOK, 256), BF16),
            pltpu.VMEM((TOK, 256), BF16),
            pltpu.VMEM((TOK, 256), BF16),
            pltpu.VMEM((TOK, 256), BF16),
            pltpu.VMEM((ALL, LANES), F32),
            sem((11,)),
            sem((SEMS,)),
            sem((SEMS,)),
        ],
        compiler_params=pltpu.CompilerParams(
            collective_id=0, has_side_effects=True, vmem_limit_bytes=58 * 1024 * 1024
        ),
    )(
        inputs, cotangent, gate_pre.T, up_pre.T,
        down_weight.T, gate_weight.T, up_weight.T, gate_scale, up_scale, down_scale,
    )
    oi, og, ou, od = pl.pallas_call(
        hand_out,
        out_shape=(
            jax.ShapeDtypeStruct((TOK, 256), BF16),
            jax.ShapeDtypeStruct((FFL, LANES), F32),
            jax.ShapeDtypeStruct((FFL, LANES), F32),
            jax.ShapeDtypeStruct((FFL, LANES), F32),
        ),
        in_specs=[hbm] * 2,
        out_specs=(hbm,) * 4,
        scratch_shapes=[
            pltpu.VMEM((TOK, 256), BF16), pltpu.VMEM((ALL, LANES), F32), sem((4,)), sem((4,)),
        ],
        compiler_params=pltpu.CompilerParams(vmem_limit_bytes=60 * 1024 * 1024),
    )(oi, out)
    return oi, og.T, ou.T, od.T


def solution(mesh):
    rows = ("rep", "fs")
    in_specs = (
        P(rows, None), P(rows, None), P(rows, "tp"), P(rows, "tp"),
        P("fs", "tp"), P("fs", "tp"), P("fs", "tp"),
        P(None, "tp"), P(None, "tp"), P(None, "tp"),
    )
    out_specs = (P(rows, "tp"), P("fs", "tp"), P("fs", "tp"), P("fs", "tp"))
    return jax.shard_map(local, mesh=mesh, in_specs=in_specs, out_specs=out_specs, check_vma=False)
```
